256 devices in a mesh: sp: 32 (over z, x), tp: 8 (over y, core).
Axes of the slice: x: 4, y: 4, z: 8, core: 2. Of those that a mesh axis runs over, the one named last changes fastest.
Arguments:
- tokens_in: bfloat16 [8192, 2048], P(('sp', 'tp')), may hold values from -128 to 128
- norm_gain: float32 [2048], replicated, may hold values from 0.1 to 1.9
- w_recept: bfloat16 [2048, 1024], P(None, 'tp'), may hold values from -0.125 to 0.125
- w_key_lin: bfloat16 [2048, 1024], P(None, 'tp'), may hold values from -0.125 to 0.125
- w_value_lin: bfloat16 [2048, 1024], P(None, 'tp'), may hold values from -0.125 to 0.125
- w_decay: bfloat16 [2048, 1024], P(None, 'tp'), may hold values from -0.125 to 0.125
- w_removal: bfloat16 [2048, 1024], P(None, 'tp'), may hold values from -0.125 to 0.125
- decay_base: float32 [1024], P('tp'), may hold values from -16 to -2.5
- removal_base: float32 [1024], P('tp'), may hold values from -8 to 1.5
- decay_extra: float32 [8192, 1024], P('sp', 'tp'), may hold values from -3 to 0
- initial_state: float32 [16, 64, 64], P('tp'), may hold values from -3072 to 3072
- group_gain: float32 [1024], P('tp'), may hold values from 0.1 to 1.9
- w_query: bfloat16 [2048, 1024], P(None, 'tp'), may hold values from -2 to 2
- w_key_win: bfloat16 [2048, 512], P(None, 'tp'), may hold values from -2 to 2
- w_value_win: bfloat16 [2048, 512], P(None, 'tp'), may hold values from -0.125 to 0.125
- sink_logit: float32 [16], P('tp'), may hold values from 3 to 7
- w_out_linear: bfloat16 [1024, 2048], P('tp'), may hold values from -0.1875 to 0.1875
- w_out_window: bfloat16 [1024, 2048], P('tp'), may hold values from -1 to 1
Outputs:
- mixed: bfloat16 [8192, 2048], P(('sp', 'tp'))
The draws below stay inside these ranges and needn't reach their ends.
All inputs are finite; a program needn't handle non-finite values.
Results may differ from the reference program's by a relative error of at most 0.017.
Values may be sent and summed in bfloat16 or wider, within the bound.
No kernel may reach another device: no remote copies, remote signals or barrier semaphores. Data moves between devices by JAX's collectives and lax.ppermute only.
A program may use at most 64 MiB of HBM per device.

```python
import math
import jax
import jax.numpy as jnp
from jax import lax

D = 2048
HEAD_CHANNELS = 64
RECURRENT_HEADS = 16
AQ = 16
AKV = 8
WINDOW = 128
RW = 1024
AW = 1024
SEQUENCE_TOKENS = 8192
N_TP = 8


def attention_pair(key):
    query_w = jnp.clip(jax.random.normal(jax.random.fold_in(key, 101), (D, AQ * HEAD_CHANNELS), jnp.float32), -6.0, 6.0) * D ** (-0.5)
    key_w = jnp.clip(jax.random.normal(jax.random.fold_in(key, 102), (D, AKV * HEAD_CHANNELS), jnp.float32), -6.0, 6.0) * D ** (-0.5)
    return (query_w, key_w)


def draw_w_query(key, part):
    return attention_pair(key)[0].astype(jnp.bfloat16)


def draw_w_key_win(key, part):
    return attention_pair(key)[1].astype(jnp.bfloat16)


def draw_tokens_in(key, part):
    noise = jnp.clip(jax.random.normal(jax.random.fold_in(key, 201), (SEQUENCE_TOKENS, D), jnp.float32), -6.0, 6.0)
    segment_total = (SEQUENCE_TOKENS + 63) // 64
    shared = jnp.clip(jax.random.normal(jax.random.fold_in(key, 204), (segment_total, D), jnp.float32), -6.0, 6.0)
    base = 0.4 * noise + jnp.repeat(shared, 64, axis=0)[:SEQUENCE_TOKENS]
    return base.astype(jnp.bfloat16)


def decay_parts(key):
    share = 0.5
    heads_fast = jax.random.uniform(jax.random.fold_in(key, 301), (RECURRENT_HEADS,), jnp.float32) < share
    quick_removal = jnp.repeat(heads_fast, HEAD_CHANNELS)
    slow_rate = jnp.exp(jax.random.uniform(jax.random.fold_in(key, 302), (RW,), jnp.float32, math.log(0.02), math.log(0.15))) / SEQUENCE_TOKENS
    fast_rate = jnp.exp(jax.random.uniform(jax.random.fold_in(key, 303), (RW,), jnp.float32, math.log(0.015), math.log(0.05)))
    rate = jnp.where(quick_removal, fast_rate, slow_rate)
    removal_slow = jax.random.uniform(jax.random.fold_in(key, 304), (RW,), jnp.float32, math.log(0.375 * HEAD_CHANNELS), math.log(1.5 * HEAD_CHANNELS)) - math.log(SEQUENCE_TOKENS)
    removal_fast = jax.random.uniform(jax.random.fold_in(key, 305), (RW,), jnp.float32, -1.5, 1.5)
    removal_base = jnp.where(quick_removal, removal_fast, removal_slow)
    block_total = (SEQUENCE_TOKENS + 511) // 512
    block_factor = jnp.exp(jax.random.uniform(jax.random.fold_in(key, 306), (block_total,), jnp.float32, math.log(0.2), math.log(4.0)))
    position_factor = jnp.repeat(block_factor, 512)[:SEQUENCE_TOKENS]
    additional_decay = -rate[None, :] * position_factor[:, None]
    spike_position = jax.random.randint(jax.random.fold_in(key, 307), (3,), 0, SEQUENCE_TOKENS)
    spike_penalty = jax.random.uniform(jax.random.fold_in(key, 308), (3, RECURRENT_HEADS), jnp.float32, math.log(0.5), math.log(0.8))
    spike_row_list = jnp.where(quick_removal[None, :], 0.0, jnp.repeat(spike_penalty, HEAD_CHANNELS, axis=1))
    additional_decay = additional_decay.at[spike_position].add(spike_row_list)
    return (jnp.log(rate), removal_base, additional_decay)


def draw_decay_base(key, part):
    return decay_parts(key)[0]


def draw_removal_base(key, part):
    return decay_parts(key)[1]


def draw_decay_extra(key, part):
    return decay_parts(key)[2]


def levels(key, extent, shards, least, largest):
    level, own = 1.0, jax.random.fold_in(key, 6)
    for axis_at, blocks in shards:
        heights = jnp.exp(jax.random.uniform(jax.random.fold_in(own, axis_at), (blocks,), jnp.float32, least / len(shards), largest / len(shards)))
        level = level * jnp.repeat(heights, extent[axis_at] // blocks).reshape([-1 if axis == axis_at else 1 for axis in range(len(extent))])
    return level


def bell_draw(rng, extent, scale, bound, cuts=(), kind=jnp.bfloat16):
    drawn = scale * jax.random.normal(rng, extent, jnp.float32)
    if cuts:
        drawn = drawn * levels(rng, extent, cuts, -0.22, 0.18)
    return jnp.clip(drawn, -bound, bound).astype(kind)


def setup_inputs(seed: int = 0) -> dict:
    splits = jax.random.split(jax.random.key(seed), 19)
    tokens_in = draw_tokens_in(jax.random.fold_in(splits[18], 71), 0)
    norm_gain = jnp.clip(1.0 + 0.18 * jax.random.normal(splits[1], (D,), jnp.float32), 0.1, 1.9)
    w_recept = bell_draw(splits[2], (D, RW), D ** -0.5, 0.125, ((1, 8),))
    w_key_lin = bell_draw(splits[3], (D, RW), D ** -0.5, 0.125, ((1, 8),))
    w_value_lin = bell_draw(splits[4], (D, RW), D ** -0.5, 0.125, ((1, 8),))
    w_decay = bell_draw(splits[5], (D, RW), D ** -0.5, 0.125, ((1, 8),))
    w_removal = bell_draw(splits[6], (D, RW), D ** -0.5, 0.125, ((1, 8),))
    decay_base = draw_decay_base(jax.random.fold_in(splits[18], 71), 0)
    removal_base = draw_removal_base(jax.random.fold_in(splits[18], 71), 0)
    decay_extra = draw_decay_extra(jax.random.fold_in(splits[18], 71), 0)
    initial_state = bell_draw(splits[10], (RECURRENT_HEADS, HEAD_CHANNELS, HEAD_CHANNELS), (6.0 * SEQUENCE_TOKENS ** 0.5), 3072.0, ((0, 8),), jnp.float32)
    group_gain = jnp.clip(1.0 + 0.18 * jax.random.normal(splits[11], (RW,), jnp.float32), 0.1, 1.9)
    w_query = draw_w_query(jax.random.fold_in(splits[18], 71), 0)
    w_key_win = draw_w_key_win(jax.random.fold_in(splits[18], 71), 0)
    w_value_win = bell_draw(splits[14], (D, AKV * HEAD_CHANNELS), D ** -0.5, 0.125, ((1, 8),))
    sink_logit = jnp.clip(3.0 + 4.0 * jax.random.uniform(splits[15], (AQ,), jnp.float32) ** levels(splits[15], (AQ,), ((0, 8),), -0.2, 0.2), 3.0, 7.0)
    w_out_linear = bell_draw(splits[16], (RW, D), RW ** -0.5, 0.1875, ((0, 8),))
    w_out_window = bell_draw(splits[17], (AW, D), (AW // 32) ** -0.5, 1.0, ((0, 8),))
    return dict(tokens_in=tokens_in, norm_gain=norm_gain, w_recept=w_recept, w_key_lin=w_key_lin, w_value_lin=w_value_lin, w_decay=w_decay, w_removal=w_removal, decay_base=decay_base, removal_base=removal_base, decay_extra=decay_extra, initial_state=initial_state, group_gain=group_gain, w_query=w_query, w_key_win=w_key_win, w_value_win=w_value_win, sink_logit=sink_logit, w_out_linear=w_out_linear, w_out_window=w_out_window)


rms_eps = 1e-06
group_eps = 0.00064
key_eps = 1e-06
theta_base = 10000.0
highest_precision = lax.Precision.HIGHEST

def rotate(values, positions):
    half = HEAD_CHANNELS // 2
    inverse = theta_base ** (-jnp.arange(0, HEAD_CHANNELS, 2, dtype=jnp.float32) / HEAD_CHANNELS)
    angle = positions[:, None, None] * inverse
    cosine = jnp.cos(angle)
    sine = jnp.sin(angle)
    first = values[..., :half]
    second = values[..., half:]
    return jnp.concatenate([first * cosine - second * sine, second * cosine + first * sine], axis=-1)

def advance(state, inputs):
    read_vec, decay_vec, key_vec, value_vec, unit_vec, strike_vec = inputs
    erased = jnp.einsum('hvk,hk->hv', state, unit_vec, precision=highest_precision)
    state = state * decay_vec[:, None, :] - erased[:, :, None] * strike_vec[:, None, :] + value_vec[:, :, None] * key_vec[:, None, :]
    return (state, jnp.einsum('hvk,hk->hv', state, read_vec, precision=highest_precision))

def window_head(inputs):
    query_block_list, key_blocks, value_blocks, sinks = inputs
    block_count = query_block_list.shape[0]
    zeros_block = jnp.zeros_like(key_blocks[:1])
    banded_key = jnp.concatenate([jnp.concatenate([zeros_block, key_blocks[:-1]], axis=0), key_blocks], axis=1)
    banded_value = jnp.concatenate([jnp.concatenate([zeros_block, value_blocks[:-1]], axis=0), value_blocks], axis=1)
    attention_scores = jnp.einsum('eima,ela->emil', query_block_list.astype(jnp.float32), banded_key.astype(jnp.float32), precision=highest_precision)
    q_index = jnp.arange(WINDOW)
    k_index = jnp.arange(2 * WINDOW)
    relative = WINDOW + q_index[:, None] - k_index[None, :]
    near = (relative >= 0) & (relative < WINDOW)
    key_pos = (jnp.arange(block_count)[:, None] - 1) * WINDOW + k_index[None, :]
    valid_mask = near[None, :, :] & (key_pos >= 0)[:, None, :]
    attention_scores = jnp.where(valid_mask[:, None, :, :], attention_scores, -jnp.inf)
    sink_col = sinks[None, :, None, None]
    row_top = jnp.maximum(lax.optimization_barrier(jnp.max(attention_scores, axis=-1, keepdims=True)), sink_col)
    raised = jnp.exp(attention_scores - row_top)
    row_total = lax.optimization_barrier(jnp.sum(raised, axis=-1, keepdims=True)) + jnp.exp(sink_col - row_top)
    attention_probability = (raised / row_total).astype(jnp.bfloat16)
    return jnp.einsum('wozm,wmr->wzor', attention_probability.astype(jnp.float32), banded_value.astype(jnp.float32), precision=highest_precision)

def reference(tokens_in, norm_gain, w_recept, w_key_lin, w_value_lin, w_decay, w_removal, decay_base, removal_base, decay_extra, initial_state, group_gain, w_query, w_key_win, w_value_win, sink_logit, w_out_linear, w_out_window):
    wide = tokens_in.astype(jnp.float32)
    normed = (wide * lax.rsqrt(lax.optimization_barrier(jnp.mean(wide * wide, axis=-1, keepdims=True)) + rms_eps) * norm_gain).astype(jnp.bfloat16)

    def project(weight):
        return jnp.dot(normed, weight, preferred_element_type=jnp.float32).astype(jnp.bfloat16)
    receptance = project(w_recept)
    lin_key = project(w_key_lin)
    lin_value = project(w_value_lin)
    decay_pre = project(w_decay)
    removal_pre = project(w_removal)
    query_rows = project(w_query)
    key_rows = project(w_key_win)
    value_rows = project(w_value_win)
    head_shape = (SEQUENCE_TOKENS, RECURRENT_HEADS, HEAD_CHANNELS)
    recept_f = receptance.astype(jnp.float32).reshape(head_shape)
    key_full = lin_key.astype(jnp.float32).reshape(head_shape)
    value_full = lin_value.astype(jnp.float32).reshape(head_shape)
    log_decay = -jnp.exp(decay_base + decay_pre.astype(jnp.float32)) + decay_extra
    decays = jnp.exp(log_decay).reshape(head_shape)
    removal = jax.nn.sigmoid(removal_base + removal_pre.astype(jnp.float32)).reshape(head_shape)
    unit_key = key_full * lax.rsqrt(lax.optimization_barrier(jnp.sum(key_full * key_full, axis=-1, keepdims=True)) + key_eps)
    strike = unit_key * removal
    final_state, lin_read = lax.scan(advance, initial_state, (recept_f, decays, key_full, value_full, unit_key, strike))
    centered = lin_read - lax.optimization_barrier(jnp.mean(lin_read, axis=-1, keepdims=True))
    spread = lax.optimization_barrier(jnp.mean(centered * centered, axis=-1, keepdims=True))
    lin_out = (centered * lax.rsqrt(spread + group_eps) * group_gain.reshape(RECURRENT_HEADS, HEAD_CHANNELS)).reshape(SEQUENCE_TOKENS, RW).astype(jnp.bfloat16)
    positions = jnp.arange(SEQUENCE_TOKENS).astype(jnp.float32)
    query_rot = (rotate(query_rows.astype(jnp.float32).reshape(SEQUENCE_TOKENS, AQ, HEAD_CHANNELS), positions) * HEAD_CHANNELS ** (-0.5)).astype(jnp.bfloat16)
    key_rot = rotate(key_rows.astype(jnp.float32).reshape(SEQUENCE_TOKENS, AKV, HEAD_CHANNELS), positions).astype(jnp.bfloat16)
    group_size = AQ // AKV
    block_count = SEQUENCE_TOKENS // WINDOW
    query_heads = jnp.moveaxis(query_rot.reshape(block_count, WINDOW, AKV, group_size, HEAD_CHANNELS), 2, 0)
    key_heads = jnp.moveaxis(key_rot.reshape(block_count, WINDOW, AKV, HEAD_CHANNELS), 2, 0)
    value_heads = jnp.moveaxis(value_rows.reshape(block_count, WINDOW, AKV, HEAD_CHANNELS), 2, 0)
    sink_heads = sink_logit.reshape(AKV, group_size)
    head_outs = lax.map(window_head, (query_heads, key_heads, value_heads, sink_heads))
    win_out = jnp.transpose(head_outs, (1, 2, 0, 3, 4)).reshape(SEQUENCE_TOKENS, AW).astype(jnp.bfloat16)
    lin_group = RW // N_TP
    win_group = AW // N_TP
    total = jnp.zeros((SEQUENCE_TOKENS, D), jnp.float32)
    for group_index in range(N_TP):
        lin_cols = lin_out[:, group_index * lin_group:(group_index + 1) * lin_group]
        win_cols = win_out[:, group_index * win_group:(group_index + 1) * win_group]
        term = jnp.dot(lin_cols, w_out_linear[group_index * lin_group:(group_index + 1) * lin_group], preferred_element_type=jnp.float32)
        term = term + jnp.dot(win_cols, w_out_window[group_index * win_group:(group_index + 1) * win_group], preferred_element_type=jnp.float32)
        rounded = lax.optimization_barrier(term.astype(jnp.bfloat16))
        total = total + rounded.astype(jnp.float32)
    return total.astype(jnp.bfloat16)
```

```python
import jax
import jax.numpy as jnp
from jax import lax
from jax.experimental import pallas as pl
from jax.experimental.pallas import tpu as pltpu
from jax.sharding import Mesh
from jax.sharding import PartitionSpec as P

HC = 64
WINDOW = 128
CH = 64
LANES = 128
SP = ("z", "x")
TP = ("y", "c")

rms_eps = 1e-06
group_eps = 0.00064
key_eps = 1e-06
theta_base = 10000.0
F32 = jnp.float32
BF16 = jnp.bfloat16

NN = (((1,), (0,)), ((), ()))
NT = (((1,), (1,)), ((), ()))
TN = (((0,), (0,)), ((), ()))


def dot1(a, b, dims=NN):
    return lax.dot_general(a.astype(BF16), b.astype(BF16), dims, preferred_element_type=F32)


def split(a):
    high = a.astype(BF16)
    return high, (a - high.astype(F32)).astype(BF16)


def dot3(a, b, dims=NN):
    ah, al = split(a)
    bh, bl = split(b)
    d = lambda p, q: lax.dot_general(p, q, dims, preferred_element_type=F32)
    return d(ah, bh) + (d(ah, bl) + d(al, bh))


dot_pair = dot3
dot_inv = dot3
dot_map = dot3


def head_masks(rows):
    lane = lax.broadcasted_iota(jnp.int32, (rows, LANES), 1)
    first = lane < HC
    return first


def stack2(a):
    first = head_masks(a.shape[0])
    zero = jnp.zeros_like(a)
    return jnp.concatenate([jnp.where(first, a, zero), jnp.where(first, zero, a)], axis=0)


def fold2(a):
    half = a.shape[0] // 2
    return a[:half] + a[half:]


def head_sum(a):
    first = head_masks(a.shape[0])
    low = jnp.sum(jnp.where(first, a, 0.0), axis=-1, keepdims=True)
    high = jnp.sum(jnp.where(first, 0.0, a), axis=-1, keepdims=True)
    return jnp.where(first, low, high)


def eye(count):
    row = lax.broadcasted_iota(jnp.int32, (count, count), 0)
    col = lax.broadcasted_iota(jnp.int32, (count, count), 1)
    return row == col


def level_mask(half):
    row = lax.broadcasted_iota(jnp.int32, (LANES, LANES), 0)
    col = lax.broadcasted_iota(jnp.int32, (LANES, LANES), 1)
    step = 2 * half
    same = (row // step) == (col // step)
    return same & ((row % step) >= half) & ((col % step) < half)


class Decays:
    def __init__(self, decay):
        rows = decay.shape[0]
        self.row = lax.broadcasted_iota(jnp.int32, decay.shape, 0)
        self.rows = rows
        self.half = 1
        self.incl = decay
        self.excl = jnp.ones_like(decay)
        self.tail = jnp.ones_like(decay)
        self.total = decay

    def widen(self):
        h = self.half
        second = (self.row % (2 * h)) >= h
        back = pltpu.roll(self.total, h, 0)
        ahead = pltpu.roll(self.total, self.rows - h, 0)
        sibling = jnp.where(second, back, ahead)
        lead = jnp.where(second, sibling, 1.0)
        self.incl = self.incl * lead
        self.excl = self.excl * lead
        self.tail = self.tail * jnp.where(second, 1.0, sibling)
        self.total = self.total * sibling
        self.half = 2 * h


def lin_map_kernel(
    same_ref, other_ref, gain_ref, wk_ref, wv_ref, wd_ref, wr_ref,
    db_ref, rb_ref, extra_ref, core_ref,
    normed_ref, key_ref, value_ref, strike_ref, decay_ref, sol_ref, pre_ref, map_ref,
):
    core = core_ref[0]
    count = same_ref.shape[0]
    rows = same_ref.shape[1]
    gain = gain_ref[...]
    for j in range(count):
        for ref, which in ((same_ref, core), (other_ref, 1 - core)):
            wide = ref[j].astype(F32)
            scale = lax.rsqrt(jnp.mean(wide * wide, axis=-1, keepdims=True) + rms_eps)
            at = pl.multiple_of((2 * j + which) * rows, rows)
            normed_ref[pl.ds(at, rows), :] = (wide * scale * gain).astype(BF16)
    normed = normed_ref[...]

    def project(ref):
        return jnp.dot(normed, ref[...], preferred_element_type=F32).astype(BF16)

    key_b = project(wk_ref)
    value_b = project(wv_ref)
    decay_pre = project(wd_ref).astype(F32)
    removal_pre = project(wr_ref).astype(F32)
    key = key_b.astype(F32)
    value = value_b.astype(F32)
    decay = jnp.exp(-jnp.exp(db_ref[...] + decay_pre) + extra_ref[...])
    removal = jax.nn.sigmoid(rb_ref[...] + removal_pre)
    unit = key * lax.rsqrt(head_sum(key * key) + key_eps)
    strike = unit * removal
    key_ref[...] = key_b
    value_ref[...] = value_b
    strike_ref[...] = strike
    decay_ref[...] = decay

    chunks = normed.shape[0] // CH
    ident = eye(LANES)
    prefix = None
    for b in range(chunks):
        part = slice(b * CH, (b + 1) * CH)
        u, s, k, v = -unit[part], strike[part], key[part], value[part]
        dec = Decays(decay[part])
        inverse = jnp.where(ident, 1.0, 0.0).astype(F32)
        mix_key = jnp.zeros((LANES, LANES), F32)
        while dec.half < CH:
            left = stack2(u * dec.excl)
            st = s * dec.tail
            kt = k * dec.tail
            pairs = dot_pair(left, jnp.concatenate([st, st, kt, kt], axis=0), NT)
            mask = level_mask(dec.half)
            lower = jnp.where(mask, pairs[:, :LANES], 0.0)
            mix_key = jnp.where(mask, pairs[:, LANES:], mix_key)
            if dec.half == 1:
                inverse = inverse + lower
            else:
                inverse = inverse + dot_inv(inverse, dot_inv(lower, inverse))
            dec.widen()
        v2 = stack2(v)
        right = jnp.concatenate([stack2(u * dec.excl), dot_map(mix_key, v2)], axis=1)
        sol = dot_map(inverse, right)
        sol_ref[b] = sol
        strike_tail = stack2(s * dec.tail)
        key_tail = stack2(k * dec.tail)
        both = dot_map(sol, strike_tail, TN)
        trans = both[:LANES] + jnp.where(ident, dec.total[0:1], 0.0)
        add = both[LANES:] + dot_map(v2, key_tail, TN)
        if b == 0:
            prefix = jnp.concatenate([trans, add], axis=0)
        else:
            pre_ref[b - 1] = prefix
            prefix = dot_map(prefix, trans) + jnp.concatenate([jnp.zeros_like(add), add], axis=0)
    map_ref[...] = jnp.concatenate([fold2(prefix[:LANES]), fold2(prefix[LANES:])], axis=0)


def rope(values, cosine, sine):
    lane = lax.broadcasted_iota(jnp.int32, values.shape, 1)
    low = (lane % HC) < HC // 2
    ahead = pltpu.roll(values, LANES - HC // 2, 1)
    back = pltpu.roll(values, HC // 2, 1)
    return values * cosine + jnp.where(low, -ahead, back) * sine


def qkv_kernel(normed_ref, wq_ref, wkv_ref, cos_ref, sin_ref, q_ref, kv_ref):
    normed = normed_ref[...]
    cosine = cos_ref[...]
    sine = sin_ref[...]
    q = jnp.dot(normed, wq_ref[...], preferred_element_type=F32).astype(BF16).astype(F32)
    q_ref[...] = (rope(q, cosine, sine) * HC ** (-0.5)).astype(BF16)
    kv_b = jnp.dot(normed, wkv_ref[...], preferred_element_type=F32).astype(BF16)
    kv = kv_b.astype(F32)
    first = head_masks(kv.shape[0])
    kv_ref[...] = jnp.where(first, rope(kv, cosine, sine), kv).astype(BF16)


def read_kernel(
    normed_ref, wrec_ref, key_ref, value_ref, strike_ref, decay_ref, sol_ref, pre_ref,
    base_ref, read_ref,
):
    normed = normed_ref[...]
    recept = jnp.dot(normed, wrec_ref[...], preferred_element_type=F32).astype(BF16).astype(F32)
    key = key_ref[...].astype(F32)
    value = value_ref[...].astype(F32)
    strike = strike_ref[...]
    decay = decay_ref[...]
    ident = eye(LANES)
    for b in range(normed.shape[0] // CH):
        part = slice(b * CH, (b + 1) * CH)
        r, s, k, v = recept[part], strike[part], key[part], value[part]
        dec = Decays(decay[part])
        pairs = dot_pair(stack2(r), jnp.concatenate([s, s, k, k], axis=0), NT)
        out_beta = jnp.where(ident, pairs[:, :LANES], 0.0)
        out_key = jnp.where(ident, pairs[:, LANES:], 0.0)
        while dec.half < CH:
            st = s * dec.tail
            kt = k * dec.tail
            pairs = dot_pair(stack2(r * dec.incl), jnp.concatenate([st, st, kt, kt], axis=0), NT)
            mask = level_mask(dec.half)
            out_beta = jnp.where(mask, pairs[:, :LANES], out_beta)
            out_key = jnp.where(mask, pairs[:, LANES:], out_key)
            dec.widen()
        both = dot_map(out_beta, sol_ref[b])
        read = stack2(r * dec.incl) + both[:, :LANES]
        local = both[:, LANES:] + dot_map(out_key, stack2(v))
        if b == 0:
            read_ref[part, :] = fold2(read)
            base_ref[part, :] = fold2(local)
        else:
            through = dot_map(read, pre_ref[b - 1], NT)
            read_ref[part, :] = fold2(through[:, :LANES])
            base_ref[part, :] = fold2(through[:, LANES:] + local)


def window_kernel(q_ref, kv_ref, rim_ref, sink_ref, start_ref, out_ref):
    q_all = q_ref[...].astype(F32)
    kv_all = kv_ref[...]
    first = head_masks(WINDOW)
    seen = start_ref[0]
    row = lax.broadcasted_iota(jnp.int32, (2 * WINDOW, 2 * WINDOW), 0) % WINDOW
    col = lax.broadcasted_iota(jnp.int32, (2 * WINDOW, 2 * WINDOW), 1)
    relative = WINDOW + row - col
    near = (relative >= 0) & (relative < WINDOW)
    head = lax.broadcasted_iota(jnp.int32, (2 * WINDOW, 1), 0) < WINDOW
    sinks = jnp.where(head, sink_ref[0], sink_ref[1])
    for b in range(q_all.shape[0] // WINDOW):
        q = q_all[b * WINDOW : (b + 1) * WINDOW]
        shifted = pltpu.roll(q, HC, 1)
        left = jnp.concatenate(
            [jnp.where(first, q, 0.0), jnp.where(first, shifted, 0.0)], axis=0
        ).astype(BF16)
        if b == 0:
            keys = jnp.concatenate([rim_ref[...], kv_all[:WINDOW]], axis=0)
            valid = near & (col >= seen)
        else:
            keys = kv_all[(b - 1) * WINDOW : (b + 1) * WINDOW]
            valid = near
        scores = lax.dot_general(left, keys, NT, preferred_element_type=F32)
        scores = jnp.where(valid, scores, -jnp.inf)
        top = jnp.maximum(jnp.max(scores, axis=-1, keepdims=True), sinks)
        raised = jnp.exp(scores - top)
        total = jnp.sum(raised, axis=-1, keepdims=True) + jnp.exp(sinks - top)
        prob = (raised / total).astype(BF16)
        weighted = jnp.dot(prob, keys, preferred_element_type=F32)
        low = pltpu.roll(weighted[:WINDOW], HC, 1)
        out_ref[b * WINDOW : (b + 1) * WINDOW, :] = jnp.where(
            first, low, weighted[WINDOW:]
        ).astype(BF16)


def join_kernel(maps_ref, at_ref, total_ref, before_ref):
    at = at_ref[0]
    count = maps_ref.shape[0]

    def expand(k):
        both = maps_ref[k]
        return jnp.concatenate([stack2(both[:HC]), stack2(both[HC:])], axis=0)

    total = expand(0)
    ident = jnp.where(eye(LANES), 1.0, 0.0).astype(F32)
    before = jnp.concatenate([ident, jnp.zeros_like(ident)], axis=0)
    for k in range(1, count):
        before = jnp.where(at >= k, total, before)
        later = expand(k)
        total = dot_map(total, later[:LANES])
        total = total + jnp.concatenate([jnp.zeros_like(ident), later[LANES:]], axis=0)
    before_ref[...] = before
    total_ref[...] = jnp.concatenate(
        [fold2(total[:LANES]), fold2(total[LANES:])], axis=0
    ).astype(BF16)


def final_kernel(
    maps_ref, at_ref, core_ref, before_ref, state_ref, base_ref, read_ref, gain_ref, win_ref,
    wl_ref, ww_ref, same_ref, other_ref,
):
    at = at_ref[0]
    core = core_ref[0]
    state = state_ref[...]
    for k in range(maps_ref.shape[0] - 1):
        both = maps_ref[k]
        high, low = split(state)
        moved = lax.dot_general(
            jnp.concatenate([high, low], axis=0), stack2(both[:HC]), NN,
            preferred_element_type=F32,
        )
        moved = moved[:LANES] + moved[LANES:] + stack2(both[HC:].astype(F32))
        state = jnp.where(at > k, moved, state)
    state = dot_map(state, before_ref[:LANES, :]) + before_ref[LANES:, :]
    reading = base_ref[...] + dot_map(read_ref[...], state, NT)
    centered = reading - head_sum(reading) * (1.0 / HC)
    spread = head_sum(centered * centered) * (1.0 / HC)
    lin = (centered * lax.rsqrt(spread + group_eps) * gain_ref[...]).astype(BF16)
    left = jnp.concatenate([lin, win_ref[...]], axis=1)
    weights = jnp.concatenate([wl_ref[...], ww_ref[...]], axis=0)
    term = jnp.dot(left, weights, preferred_element_type=F32).astype(BF16)
    blocks = same_ref.shape[0]
    rows = same_ref.shape[1]
    for j in range(blocks):
        even = term[2 * j * rows : (2 * j + 1) * rows]
        odd = term[(2 * j + 1) * rows : (2 * j + 2) * rows]
        same_ref[j] = jnp.where(core == 0, even, odd)
        other_ref[j] = jnp.where(core == 0, odd, even)


VM = pl.BlockSpec(memory_space=pltpu.VMEM)
SM = pl.BlockSpec(memory_space=pltpu.SMEM)


def call(kernel, outs, args, smem=(), name=None, flops=1e9):
    specs = [SM if i in smem else VM for i in range(len(args))]
    return pl.pallas_call(
        kernel,
        out_shape=outs,
        in_specs=specs,
        out_specs=jax.tree.map(lambda _: VM, outs),
        name=name,
        cost_estimate=pl.CostEstimate(flops=int(flops), transcendentals=0, bytes_accessed=1000000),
    )(*args)


def shape(dims, dtype):
    return jax.ShapeDtypeStruct(dims, dtype)


def exchanged(array, axis):
    return lax.all_to_all(array, axis, split_axis=0, concat_axis=0, tiled=True)


def copies(array, axis):
    return jnp.broadcast_to(array, (lax.axis_size(axis), *array.shape))


def per_device(
    tokens_in, norm_gain, w_recept, w_key_lin, w_value_lin, w_decay, w_removal,
    decay_base, removal_base, decay_extra, initial_state, group_gain,
    w_query, w_key_win, w_value_win, sink_logit, w_out_linear, w_out_window,
):
    model = tokens_in.shape[1]
    count = decay_extra.shape[0]
    width = decay_extra.shape[1]
    chunks = count // CH
    core = lax.axis_index("c").astype(jnp.int32).reshape(1)
    at_x = lax.axis_index("x").astype(jnp.int32).reshape(1)
    at_z = lax.axis_index("z").astype(jnp.int32).reshape(1)
    sp_index = lax.axis_index(SP)
    swap = [(0, 1), (1, 0)]

    same = exchanged(copies(tokens_in, "y"), "y")
    other = lax.ppermute(same, "c", swap)

    inverse = theta_base ** (-jnp.arange(0, HC, 2, dtype=F32) / HC)
    positions = (sp_index * count + jnp.arange(count)).astype(F32)
    angle = positions[:, None] * jnp.tile(inverse, LANES // (HC // 2))[None, :]
    cosine = jnp.cos(angle)
    sine = jnp.sin(angle)
    w_kv = jnp.concatenate([w_key_win, w_value_win], axis=1)
    zeros = jnp.zeros((HC, HC), F32)
    state0 = jnp.concatenate(
        [
            jnp.concatenate([initial_state[0], zeros], axis=1),
            jnp.concatenate([zeros, initial_state[1]], axis=1),
        ],
        axis=0,
    )

    row = lambda a: a.reshape(1, -1)
    normed, key, value, strike, decay, sol, pre, own_map = call(
        lin_map_kernel,
        (
            shape((count, model), BF16),
            shape((count, width), BF16),
            shape((count, width), BF16),
            shape((count, width), F32),
            shape((count, width), F32),
            shape((chunks, LANES, 2 * LANES), F32),
            shape((chunks - 1, 2 * LANES, LANES), F32),
            shape((2 * HC, LANES), F32),
        ),
        (
            same, other, row(norm_gain), w_key_lin, w_value_lin, w_decay, w_removal,
            row(decay_base), row(removal_base), decay_extra, core,
        ),
        smem=(10,),
        name="lin_map",
    )
    maps_x = exchanged(copies(own_map, "x"), "x")

    q_rot, kv = call(
        qkv_kernel,
        (shape((count, LANES), BF16), shape((count, LANES), BF16)),
        (normed, w_query, w_kv, cosine, sine),
        name="qkv",
    )
    steps = lax.axis_size("z") * lax.axis_size("x")
    rim = lax.ppermute(kv[count - WINDOW :], SP, [(i, i + 1) for i in range(steps - 1)])

    total, before = call(
        join_kernel,
        (shape((2 * HC, LANES), BF16), shape((2 * LANES, LANES), F32)),
        (maps_x, at_x),
        smem=(1,),
        name="join",
    )
    maps_z = exchanged(copies(total, "z"), "z")

    base, read = call(
        read_kernel,
        (shape((count, LANES), F32), shape((count, LANES), F32)),
        (normed, w_recept, key, value, strike, decay, sol, pre),
        name="read",
    )
    start = jnp.where(sp_index == 0, WINDOW, 0).astype(jnp.int32).reshape(1)
    win = call(
        window_kernel,
        shape((count, LANES), BF16),
        (q_rot, kv, rim, sink_logit, start),
        smem=(3, 4),
        name="window",
    )
    blocks = same.shape[0]
    rows = same.shape[1]
    mine, theirs = call(
        final_kernel,
        (shape((blocks, rows, model), BF16), shape((blocks, rows, model), BF16)),
        (
            maps_z, at_z, core, before, state0, base, read, row(group_gain), win,
            w_out_linear, w_out_window,
        ),
        smem=(1, 2),
        name="final",
    )
    got = lax.ppermute(theirs, "c", swap)
    pair = (mine.astype(F32) + got.astype(F32)).astype(BF16)
    arrived = exchanged(pair, "y")
    return arrived.astype(F32).sum(axis=0).astype(BF16)


def solution(mesh):
    grid = Mesh(mesh.devices.reshape(8, 4, 4, 2), ("z", "x", "y", "c"))
    return jax.shard_map(
        per_device,
        mesh=grid,
        in_specs=(
            P((*SP, *TP), None),
            P(),
            P(None, TP),
            P(None, TP),
            P(None, TP),
            P(None, TP),
            P(None, TP),
            P(TP),
            P(TP),
            P(SP, TP),
            P(TP, None, None),
            P(TP),
            P(None, TP),
            P(None, TP),
            P(None, TP),
            P(TP),
            P(TP, None),
            P(TP, None),
        ),
        out_specs=P((*SP, *TP), None),
        check_vma=False,
    )
```

```python
import jax
import jax.numpy as jnp
from jax import lax
from jax.experimental import pallas as pl
from jax.experimental.pallas import tpu as pltpu
from jax.sharding import Mesh
from jax.sharding import PartitionSpec as P

HC = 64
WINDOW = 128
CH = 64
LANES = 128
SP = ("z", "x")
TP = ("y", "c")

rms_eps = 1e-06
group_eps = 0.00064
key_eps = 1e-06
theta_base = 10000.0
F32 = jnp.float32
BF16 = jnp.bfloat16

NN = (((1,), (0,)), ((), ()))
NT = (((1,), (1,)), ((), ()))
TN = (((0,), (0,)), ((), ()))


def dot1(a, b, dims=NN):
    return lax.dot_general(a.astype(BF16), b.astype(BF16), dims, preferred_element_type=F32)


def split(a):
    high = a.astype(BF16)
    return high, (a - high.astype(F32)).astype(BF16)


def dot3(a, b, dims=NN):
    ah, al = split(a)
    bh, bl = split(b)
    d = lambda p, q: lax.dot_general(p, q, dims, preferred_element_type=F32)
    return d(ah, bh) + (d(ah, bl) + d(al, bh))


dot_pair = dot1
dot_inv = dot1
dot_map = dot3


def head_masks(rows):
    lane = lax.broadcasted_iota(jnp.int32, (rows, LANES), 1)
    first = lane < HC
    return first


def stack2(a):
    first = head_masks(a.shape[0])
    zero = jnp.zeros_like(a)
    return jnp.concatenate([jnp.where(first, a, zero), jnp.where(first, zero, a)], axis=0)


def fold2(a):
    half = a.shape[0] // 2
    return a[:half] + a[half:]


def head_sum(a):
    first = head_masks(a.shape[0])
    low = jnp.sum(jnp.where(first, a, 0.0), axis=-1, keepdims=True)
    high = jnp.sum(jnp.where(first, 0.0, a), axis=-1, keepdims=True)
    return jnp.where(first, low, high)


def eye(count):
    row = lax.broadcasted_iota(jnp.int32, (count, count), 0)
    col = lax.broadcasted_iota(jnp.int32, (count, count), 1)
    return row == col


def level_mask(half):
    row = lax.broadcasted_iota(jnp.int32, (LANES, LANES), 0)
    col = lax.broadcasted_iota(jnp.int32, (LANES, LANES), 1)
    step = 2 * half
    same = (row // step) == (col // step)
    return same & ((row % step) >= half) & ((col % step) < half)


class Decays:
    def __init__(self, decay):
        rows = decay.shape[0]
        self.row = lax.broadcasted_iota(jnp.int32, decay.shape, 0)
        self.rows = rows
        self.half = 1
        self.incl = decay
        self.excl = jnp.ones_like(decay)
        self.tail = jnp.ones_like(decay)
        self.total = decay

    def widen(self):
        h = self.half
        second = (self.row % (2 * h)) >= h
        back = pltpu.roll(self.total, h, 0)
        ahead = pltpu.roll(self.total, self.rows - h, 0)
        sibling = jnp.where(second, back, ahead)
        lead = jnp.where(second, sibling, 1.0)
        self.incl = self.incl * lead
        self.excl = self.excl * lead
        self.tail = self.tail * jnp.where(second, 1.0, sibling)
        self.total = self.total * sibling
        self.half = 2 * h


def fold_map(both):
    return jnp.concatenate([fold2(both[:LANES]), fold2(both[LANES:])], axis=0)


def unfold_map(both):
    return jnp.concatenate([stack2(both[:HC]), stack2(both[HC:])], axis=0)


def unfold_wide(both):
    return jnp.concatenate([stack2(both[:, :LANES]), stack2(both[:, LANES:])], axis=1)


def lin_map_kernel(*refs):
    pieces = refs[:8]
    gain_ref, w_ref, small_ref, extra_ref = refs[8:12]
    normed_out, kv_out, wide_out, sol_out, pre_ref, map_ref = refs[12:18]
    normed_ref, pack, wide, sol_ref, extra_buf, sem, out_sems = refs[18:]
    wide_w = extra_buf.shape[1]
    extra_move = pltpu.make_async_copy(extra_ref, extra_buf, sem)
    extra_move.start()
    rows = pieces[0].shape[0]
    at_y = lax.axis_index("y")
    core = lax.axis_index("c")
    gain = gain_ref[...]
    for j in range(len(pieces)):
        row = pieces[j][...].astype(F32)
        scale = lax.rsqrt(jnp.mean(row * row, axis=-1, keepdims=True) + rms_eps)
        source = lax.rem(at_y + (4 - j % 4), 4)
        which = core if j < 4 else 1 - core
        at = pl.multiple_of((2 * source + which) * rows, rows)
        normed_ref[pl.ds(at, rows), :] = (row * scale * gain).astype(BF16)

    def project(columns):
        out = jnp.dot(normed_ref[...], columns, preferred_element_type=F32).astype(BF16)
        return out[:, :LANES], out[:, LANES:]

    key_b, value_b = project(w_ref[:, : 2 * wide_w])
    pack[0] = key_b
    pack[1] = value_b
    stores = [
        pltpu.make_async_copy(normed_ref, normed_out, out_sems.at[3]),
        pltpu.make_async_copy(pack, kv_out, out_sems.at[0]),
    ]
    for store in stores:
        store.start()
    decay_b, removal_b = project(w_ref[:, 2 * wide_w :])
    extra_move.wait()
    key = key_b.astype(F32)
    value = value_b.astype(F32)
    decay = jnp.exp(-jnp.exp(small_ref[0:1] + decay_b.astype(F32)) + extra_buf[...])
    removal = jax.nn.sigmoid(small_ref[1:2] + removal_b.astype(F32))
    unit = key * lax.rsqrt(head_sum(key * key) + key_eps)
    strike = unit * removal
    wide[0] = strike
    wide[1] = decay
    stores.append(pltpu.make_async_copy(wide, wide_out, out_sems.at[1]))
    stores[-1].start()

    chunks = normed_ref.shape[0] // CH
    parts = [slice(b * CH, (b + 1) * CH) for b in range(chunks)]
    ident = eye(LANES)
    one = jnp.where(ident, 1.0, 0.0).astype(F32)
    dec = Decays(decay)
    inverse = [one] * chunks
    mix_key = [jnp.zeros((LANES, LANES), F32)] * chunks
    while dec.half < CH:
        left = -unit * dec.excl
        st = strike * dec.tail
        kt = key * dec.tail
        mask = level_mask(dec.half)
        lower = []
        for b, p in enumerate(parts):
            pairs = dot_pair(
                stack2(left[p]), jnp.concatenate([st[p], st[p], kt[p], kt[p]], axis=0), NT
            )
            lower.append(jnp.where(mask, pairs[:, :LANES], 0.0))
            mix_key[b] = jnp.where(mask, pairs[:, LANES:], mix_key[b])
        if dec.half == 1:
            inverse = [inverse[b] + lower[b] for b in range(chunks)]
        else:
            step = [dot_inv(lower[b], inverse[b]) for b in range(chunks)]
            inverse = [inverse[b] + dot_inv(inverse[b], step[b]) for b in range(chunks)]
        dec.widen()
    left = -unit * dec.excl
    st = strike * dec.tail
    kt = key * dec.tail
    v2 = [stack2(value[p]) for p in parts]
    pushed = [dot_map(mix_key[b], v2[b]) for b in range(chunks)]
    sol = [
        dot_map(inverse[b], jnp.concatenate([stack2(left[p]), pushed[b]], axis=1))
        for b, p in enumerate(parts)
    ]
    for b in range(chunks):
        sol_ref[b] = fold2(sol[b])
    stores.append(pltpu.make_async_copy(sol_ref, sol_out, out_sems.at[2]))
    stores[-1].start()
    trans, add = [], []
    for b, p in enumerate(parts):
        both = dot_map(sol[b], stack2(st[p]), TN)
        trans.append(both[:LANES] + jnp.where(ident, dec.total[p][0:1], 0.0))
        add.append(both[LANES:] + dot_map(v2[b], stack2(kt[p]), TN))
    prefix = jnp.concatenate([trans[0], add[0]], axis=0)
    for b in range(1, chunks):
        pre_ref[b - 1] = fold_map(prefix)
        prefix = dot_map(prefix, trans[b])
        prefix = prefix + jnp.concatenate([jnp.zeros_like(add[b]), add[b]], axis=0)
    own = fold_map(prefix).astype(map_ref.dtype)
    for j in range(map_ref.shape[0]):
        map_ref[j] = own
    for store in stores:
        store.wait()


def rope(values, cosine, sine):
    lane = lax.broadcasted_iota(jnp.int32, values.shape, 1)
    low = (lane % HC) < HC // 2
    ahead = pltpu.roll(values, LANES - HC // 2, 1)
    back = pltpu.roll(values, HC // 2, 1)
    return values * cosine + jnp.where(low, -ahead, back) * sine


def read_kernel(
    recept_ref, pack_ref, wide_ref, sol_ref, pre_ref, base_ref, read_ref,
):
    recept = recept_ref[...].astype(F32)
    key = pack_ref[0].astype(F32)
    value = pack_ref[1].astype(F32)
    strike = wide_ref[0]
    ident = eye(LANES)
    chunks = recept.shape[0] // CH
    parts = [slice(b * CH, (b + 1) * CH) for b in range(chunks)]
    out_beta = [jnp.zeros((LANES, LANES), F32)] * chunks
    out_key = [jnp.zeros((LANES, LANES), F32)] * chunks

    def fill(r, s, k, mask):
        for b, p in enumerate(parts):
            pairs = dot_pair(stack2(r[p]), jnp.concatenate([s[p], s[p], k[p], k[p]], axis=0), NT)
            out_beta[b] = jnp.where(mask, pairs[:, :LANES], out_beta[b])
            out_key[b] = jnp.where(mask, pairs[:, LANES:], out_key[b])

    dec = Decays(wide_ref[1])
    fill(recept, strike, key, ident)
    while dec.half < CH:
        fill(recept * dec.incl, strike * dec.tail, key * dec.tail, level_mask(dec.half))
        dec.widen()
    start = recept * dec.incl
    for b, p in enumerate(parts):
        both = dot_map(out_beta[b], unfold_wide(sol_ref[b]))
        read = stack2(start[p]) + both[:, :LANES]
        local = both[:, LANES:] + dot_map(out_key[b], stack2(value[p]))
        if b == 0:
            read_ref[p, :] = fold2(read)
            base_ref[p, :] = fold2(local)
        else:
            through = dot_map(read, unfold_map(pre_ref[b - 1]), NT)
            read_ref[p, :] = fold2(through[:, :LANES])
            base_ref[p, :] = fold2(through[:, LANES:] + local)


def late_kernel(*refs):
    normed_in = refs[0]
    w_refs = refs[1:3]
    kvw_refs = refs[3:5]
    cos_ref, sin_ref = refs[5:7]
    recept_out, q_out, kv_out, rim_out, normed_ref, w_buf, kvw_buf, table, sems = refs[7:]
    width = w_refs[0].shape[1]
    narrow = kvw_refs[0].shape[0]
    moves = [(ref, kvw_buf.at[j * narrow : (j + 1) * narrow, :]) for j, ref in enumerate(kvw_refs)]
    moves += [(normed_in, normed_ref)]
    moves += [(ref, table.at[j]) for j, ref in enumerate((cos_ref, sin_ref))]
    moves += [(ref, w_buf.at[:, j * width : (j + 1) * width]) for j, ref in enumerate(w_refs)]
    moves = [pltpu.make_async_copy(a, b, sems.at[j]) for j, (a, b) in enumerate(moves)]
    for move in moves:
        move.start()
    for move in moves[:3]:
        move.wait()
    raw = lax.dot_general(normed_ref[...], kvw_buf[...], NT, preferred_element_type=F32)
    raw = raw.astype(BF16).astype(F32)
    for move in moves[3:]:
        move.wait()
    cosine = table[0]
    sine = table[1]
    kv = jnp.where(head_masks(raw.shape[0]), rope(raw, cosine, sine), raw).astype(BF16)
    kv_out[...] = kv
    rim_out[...] = kv[kv.shape[0] - WINDOW :]
    out = jnp.dot(normed_ref[...], w_buf[...], preferred_element_type=F32).astype(BF16)
    recept_out[...] = out[:, :LANES]
    q = out[:, LANES:].astype(F32)
    q_out[...] = (rope(q, cosine, sine) * HC ** (-0.5)).astype(BF16)


def window_kernel(q_ref, kv_ref, rim_ref, small_ref, out_ref):
    q_all = q_ref[...].astype(F32)
    kv_all = jnp.concatenate([rim_ref[...], kv_ref[...]], axis=0)
    first = head_masks(WINDOW)
    seen = jnp.where(lax.axis_index(SP) == 0, WINDOW, 0)
    row = lax.broadcasted_iota(jnp.int32, (2 * WINDOW, 2 * WINDOW), 0) % WINDOW
    col = lax.broadcasted_iota(jnp.int32, (2 * WINDOW, 2 * WINDOW), 1)
    relative = WINDOW + row - col
    near = (relative >= 0) & (relative < WINDOW)
    head = lax.broadcasted_iota(jnp.int32, (2 * WINDOW, 1), 0) < WINDOW
    sinks = jnp.where(head, small_ref[3:4, 0:1], small_ref[3:4, HC : HC + 1])
    for b in range(q_all.shape[0] // WINDOW):
        q = q_all[b * WINDOW : (b + 1) * WINDOW]
        shifted = pltpu.roll(q, HC, 1)
        left = jnp.concatenate(
            [jnp.where(first, q, 0.0), jnp.where(first, shifted, 0.0)], axis=0
        ).astype(BF16)
        keys = kv_all[b * WINDOW : (b + 2) * WINDOW]
        valid = near & (col >= seen) if b == 0 else near
        scores = lax.dot_general(left, keys, NT, preferred_element_type=F32)
        scores = jnp.where(valid, scores, -jnp.inf)
        top = jnp.maximum(jnp.max(scores, axis=-1, keepdims=True), sinks)
        raised = jnp.exp(scores - top)
        total = jnp.sum(raised, axis=-1, keepdims=True) + jnp.exp(sinks - top)
        prob = (raised / total).astype(BF16)
        weighted = jnp.dot(prob, keys, preferred_element_type=F32)
        low = pltpu.roll(weighted[:WINDOW], HC, 1)
        out_ref[b * WINDOW : (b + 1) * WINDOW, :] = jnp.where(
            first, low, weighted[WINDOW:]
        ).astype(BF16)


def join_kernel(maps_ref, total_ref, before_ref):
    at = lax.axis_index("x")
    count = maps_ref.shape[0]
    total = unfold_map(maps_ref[0].astype(F32))
    ident = jnp.where(eye(LANES), 1.0, 0.0).astype(F32)
    before = jnp.concatenate([ident, jnp.zeros_like(ident)], axis=0)
    for k in range(1, count):
        before = jnp.where(at >= k, total, before)
        later = unfold_map(maps_ref[k])
        high, low = split(total)
        trans = later[:LANES].astype(BF16)
        total = jnp.dot(high, trans, preferred_element_type=F32)
        total = total + jnp.dot(low, trans, preferred_element_type=F32)
        total = total + jnp.concatenate(
            [jnp.zeros_like(ident), later[LANES:].astype(F32)], axis=0
        )
    before_ref[...] = before
    folded = fold_map(total).astype(BF16)
    for j in range(total_ref.shape[0]):
        total_ref[j] = folded


def final_kernel(
    maps_ref, before_ref, state_ref, base_ref, read_ref, small_ref, win_ref,
    mine_ref, other_ref,
):
    at = lax.axis_index("z")
    core = lax.axis_index("c")
    state = state_ref[...]
    for k in range(maps_ref.shape[0] - 1):
        both = maps_ref[k]
        high, low = split(state)
        moved = lax.dot_general(
            jnp.concatenate([high, low], axis=0), stack2(both[:HC]), NN,
            preferred_element_type=F32,
        )
        moved = moved[:LANES] + moved[LANES:] + stack2(both[HC:].astype(F32))
        state = jnp.where(at > k, moved, state)
    state = dot_map(state, before_ref[:LANES, :]) + before_ref[LANES:, :]
    reading = base_ref[...] + dot_map(read_ref[...], state, NT)
    centered = reading - head_sum(reading) * (1.0 / HC)
    spread = head_sum(centered * centered) * (1.0 / HC)
    lin = (centered * lax.rsqrt(spread + group_eps) * small_ref[2:3]).astype(BF16)
    left = jnp.concatenate([lin, win_ref[...]], axis=1)
    blocks = 4
    height = left.shape[0] // (2 * blocks)
    for j in range(blocks):
        even = left[2 * j * height : (2 * j + 1) * height]
        odd = left[(2 * j + 1) * height : (2 * j + 2) * height]
        mine_ref[j * height : (j + 1) * height, :] = jnp.where(core == 0, even, odd)
        other_ref[j * height : (j + 1) * height, :] = jnp.where(core == 0, odd, even)


def out_kernel(mine_ref, got_ref, w_ref, *outs):
    at_y = lax.axis_index("y")
    height = outs[0].shape[0]
    blocks = len(outs)

    def turned(ref):
        picked = [
            ref[pl.ds(pl.multiple_of(lax.rem(at_y + d, blocks) * height, height), height), :]
            for d in range(blocks)
        ]
        return jnp.concatenate(picked, axis=0)

    left = jnp.concatenate([turned(mine_ref), turned(got_ref)], axis=1)
    term = jnp.dot(left, w_ref[...], preferred_element_type=F32).astype(BF16)
    for d in range(blocks):
        outs[d][...] = term[d * height : (d + 1) * height]


def load_columns_kernel(*refs):
    count = len(refs) - 2
    out, sems = refs[count:]
    width = refs[0].shape[1]
    moves = [
        pltpu.make_async_copy(
            refs[j], out.at[:, j * width : (j + 1) * width], sems.at[j]
        )
        for j in range(count)
    ]
    for move in moves:
        move.start()
    for move in moves:
        move.wait()


def load_rows_kernel(*refs):
    count = len(refs) - 2
    out, sems = refs[count:]
    height = refs[0].shape[0]
    moves = [
        pltpu.make_async_copy(
            refs[j], out.at[j * height : (j + 1) * height, :], sems.at[j]
        )
        for j in range(count)
    ]
    for move in moves:
        move.start()
    for move in moves:
        move.wait()


VM = pl.BlockSpec(memory_space=pltpu.VMEM)
SM = pl.BlockSpec(memory_space=pltpu.SMEM)


AN = pl.BlockSpec(memory_space=pl.ANY)


def call(kernel, outs, args, smem=(), anys=(), slow=(), any_outs=(), scratch=(), limit=16, name=None, flops=1e9):
    specs = [SM if i in smem else AN if i in anys else VM for i in range(len(args))]
    args = [
        a if i in smem else pltpu.with_memory_space_constraint(
            a, pltpu.HBM if i in anys or i in slow else pltpu.VMEM
        )
        for i, a in enumerate(args)
    ]
    return pl.pallas_call(
        kernel,
        out_shape=outs,
        in_specs=specs,
        out_specs=(
            tuple(AN if i in any_outs else VM for i in range(len(outs)))
            if isinstance(outs, tuple)
            else VM
        ),
        scratch_shapes=list(scratch),
        name=name,
        compiler_params=pltpu.CompilerParams(vmem_limit_bytes=limit << 20),
        cost_estimate=pl.CostEstimate(flops=int(flops), transcendentals=0, bytes_accessed=1000000),
    )(*args)


def shape(dims, dtype):
    return pltpu.VMEM(dims, dtype)


def exchanged(array, axis):
    return lax.all_to_all(array, axis, split_axis=0, concat_axis=0, tiled=True)


def copies(array, axis):
    return jnp.broadcast_to(array, (lax.axis_size(axis), *array.shape))


def per_device(
    tokens_in, norm_gain, w_recept, w_key_lin, w_value_lin, w_decay, w_removal,
    decay_base, removal_base, decay_extra, initial_state, group_gain,
    w_query, w_key_win, w_value_win, sink_logit, w_out_linear, w_out_window,
):
    model = tokens_in.shape[1]
    count = decay_extra.shape[0]
    width = decay_extra.shape[1]
    chunks = count // CH
    sp_index = lax.axis_index(SP)
    swap = [(0, 1), (1, 0)]
    turn = lambda array, d: lax.ppermute(array, "y", [(i, (i + d) % 4) for i in range(4)])

    near = {0: tokens_in, **{d: turn(tokens_in, d) for d in (2, 1, 3)}}
    far = {d: lax.ppermute(near[d], "c", swap) for d in (0, 2, 1, 3)}

    inverse = theta_base ** (-jnp.arange(0, HC, 2, dtype=F32) / HC)
    positions = (sp_index * count + jnp.arange(count)).astype(F32)
    angle = positions[:, None] * jnp.tile(inverse, LANES // (HC // 2))[None, :]
    cosine = jnp.cos(angle)
    sine = jnp.sin(angle)
    small = jnp.stack([decay_base, removal_base, group_gain, jnp.repeat(sink_logit, HC)])
    zeros = jnp.zeros((HC, HC), F32)
    state0 = jnp.concatenate(
        [
            jnp.concatenate([initial_state[0], zeros], axis=1),
            jnp.concatenate([zeros, initial_state[1]], axis=1),
        ],
        axis=0,
    )

    row = lambda a: a.reshape(1, -1)
    w_out_other = [lax.ppermute(w, "c", swap) for w in (w_out_linear, w_out_window)]
    w_lin = call(
        load_columns_kernel,
        shape((model, 4 * width), BF16),
        (w_key_lin, w_value_lin, w_decay, w_removal),
        anys=range(4),
        scratch=(pltpu.SemaphoreType.DMA((4,)),),
        limit=4,
        flops=3e9,
        name="load_lin",
    )
    far[2], cosine, sine, state0, w_out_other, w_lin = lax.optimization_barrier(
        (far[2], cosine, sine, state0, w_out_other, w_lin)
    )
    pieces = tuple(near[d] for d in range(4)) + tuple(far[d] for d in range(4))
    rows = tokens_in.shape[0]
    normed, kv_pack, wide, sol, pre, own_map = call(
        lin_map_kernel,
        (
            pltpu.HBM((count, model), BF16),
            pltpu.HBM((2, count, width), BF16),
            pltpu.HBM((2, count, width), F32),
            pltpu.HBM((chunks, HC, 2 * LANES), F32),
            shape((chunks - 1, 2 * HC, LANES), F32),
            shape((lax.axis_size("x"), 2 * HC, LANES), BF16),
        ),
        (*pieces, row(norm_gain), w_lin, small, decay_extra),
        anys=(11,),
        scratch=(
            pltpu.VMEM((count, model), BF16),
            pltpu.VMEM((2, count, width), BF16),
            pltpu.VMEM((2, count, width), F32),
            pltpu.VMEM((chunks, HC, 2 * LANES), F32),
            pltpu.VMEM((count, width), F32),
            pltpu.SemaphoreType.DMA,
            pltpu.SemaphoreType.DMA((4,)),
        ),
        any_outs=(0, 1, 2, 3),
        limit=12,
        name="lin_map",
    )
    maps_x = exchanged(own_map, "x")

    recept, q, kv, rim_out = call(
        late_kernel,
        (*(shape((count, width), BF16) for _ in range(3)), shape((WINDOW, width), BF16)),
        (normed, w_recept, w_query, w_key_win.T, w_value_win.T, cosine, sine),
        anys=range(7),
        scratch=(
            pltpu.VMEM((count, model), BF16),
            pltpu.VMEM((model, 2 * width), BF16),
            pltpu.VMEM((2 * w_key_win.shape[1], model), BF16),
            pltpu.VMEM((2, count, width), F32),
            pltpu.SemaphoreType.DMA((7,)),
        ),
        limit=8,
        name="late",
    )
    maps_x, rim_out = lax.optimization_barrier((maps_x, rim_out))
    steps = lax.axis_size("z") * lax.axis_size("x")
    rim = lax.ppermute(rim_out, SP, [(i, i + 1) for i in range(steps - 1)])

    total, before = call(
        join_kernel,
        (
            shape((lax.axis_size("z"), 2 * HC, LANES), BF16),
            shape((2 * LANES, LANES), F32),
        ),
        (maps_x,),
        limit=4,
        name="join",
    )
    maps_z = exchanged(total, "z")

    base, read = call(
        read_kernel,
        (shape((count, LANES), F32), shape((count, LANES), F32)),
        (recept, kv_pack, wide, sol, pre),
        slow=(1, 2, 3),
        limit=8,
        name="read",
    )
    win = call(
        window_kernel,
        shape((count, LANES), BF16),
        (q, kv, rim, small),
        limit=4,
        name="window",
    )
    mine, theirs = call(
        final_kernel,
        (shape((count // 2, 2 * LANES), BF16), shape((count // 2, 2 * LANES), BF16)),
        (maps_z, before, state0, base, read, small, win),
        limit=8,
        name="final",
    )
    mine, theirs, w_out = lax.optimization_barrier(
        (mine, theirs, (w_out_linear, w_out_window, *w_out_other))
    )
    got = lax.ppermute(theirs, "c", swap)
    w_out = call(
        load_rows_kernel,
        shape((4 * width, model), BF16),
        w_out,
        anys=range(4),
        scratch=(pltpu.SemaphoreType.DMA((4,)),),
        limit=4,
        flops=3e9,
        name="load_out",
    )
    sums = call(
        out_kernel,
        tuple(shape((rows, model), BF16) for _ in range(4)),
        (mine, got, w_out),
        limit=8,
        name="out",
    )
    arrived = [turn(sums[d], d) for d in (2, 1, 3)]
    total_rows = sums[0].astype(F32)
    for part in arrived:
        total_rows = total_rows + part.astype(F32)
    return total_rows.astype(BF16)


def solution(mesh):
    grid = Mesh(mesh.devices.reshape(8, 4, 4, 2), ("z", "x", "y", "c"))
    return jax.shard_map(
        per_device,
        mesh=grid,
        in_specs=(
            P((*SP, *TP), None),
            P(),
            P(None, TP),
            P(None, TP),
            P(None, TP),
            P(None, TP),
            P(None, TP),
            P(TP),
            P(TP),
            P(SP, TP),
            P(TP, None, None),
            P(TP),
            P(None, TP),
            P(None, TP),
            P(None, TP),
            P(TP),
            P(TP, None),
            P(TP, None),
        ),
        out_specs=P((*SP, *TP), None),
        check_vma=False,
    )
```

```python
import jax
import jax.numpy as jnp
from jax import lax
from jax.experimental import pallas as pl
from jax.experimental.pallas import tpu as pltpu
from jax.sharding import Mesh
from jax.sharding import PartitionSpec as P

HC = 64
WINDOW = 128
CH = 64
LANES = 128
SP = ("z", "x")
TP = ("y", "c")

rms_eps = 1e-06
group_eps = 0.00064
key_eps = 1e-06
theta_base = 10000.0
F32 = jnp.float32
BF16 = jnp.bfloat16

NN = (((1,), (0,)), ((), ()))
NT = (((1,), (1,)), ((), ()))
TN = (((0,), (0,)), ((), ()))


def dot1(a, b, dims=NN):
    return lax.dot_general(a.astype(BF16), b.astype(BF16), dims, preferred_element_type=F32)


def split(a):
    high = a.astype(BF16)
    return high, (a - high.astype(F32)).astype(BF16)


def dot3(a, b, dims=NN):
    ah, al = split(a)
    bh, bl = split(b)
    d = lambda p, q: lax.dot_general(p, q, dims, preferred_element_type=F32)
    return d(ah, bh) + (d(ah, bl) + d(al, bh))


dot_pair = dot1
dot_inv = dot1
dot_map = dot3


def head_masks(rows):
    lane = lax.broadcasted_iota(jnp.int32, (rows, LANES), 1)
    first = lane < HC
    return first


def stack2(a):
    first = head_masks(a.shape[0])
    zero = jnp.zeros_like(a)
    return jnp.concatenate([jnp.where(first, a, zero), jnp.where(first, zero, a)], axis=0)


def fold2(a):
    half = a.shape[0] // 2
    return a[:half] + a[half:]


def head_sum(a):
    first = head_masks(a.shape[0])
    low = jnp.sum(jnp.where(first, a, 0.0), axis=-1, keepdims=True)
    high = jnp.sum(jnp.where(first, 0.0, a), axis=-1, keepdims=True)
    return jnp.where(first, low, high)


def eye(count):
    row = lax.broadcasted_iota(jnp.int32, (count, count), 0)
    col = lax.broadcasted_iota(jnp.int32, (count, count), 1)
    return row == col


def level_mask(half):
    row = lax.broadcasted_iota(jnp.int32, (LANES, LANES), 0)
    col = lax.broadcasted_iota(jnp.int32, (LANES, LANES), 1)
    step = 2 * half
    same = (row // step) == (col // step)
    return same & ((row % step) >= half) & ((col % step) < half)


class Decays:
    def __init__(self, decay):
        rows = decay.shape[0]
        self.row = lax.broadcasted_iota(jnp.int32, decay.shape, 0)
        self.rows = rows
        self.half = 1
        self.incl = decay
        self.excl = jnp.ones_like(decay)
        self.tail = jnp.ones_like(decay)
        self.total = decay

    def widen(self):
        h = self.half
        second = (self.row % (2 * h)) >= h
        back = pltpu.roll(self.total, h, 0)
        ahead = pltpu.roll(self.total, self.rows - h, 0)
        sibling = jnp.where(second, back, ahead)
        lead = jnp.where(second, sibling, 1.0)
        self.incl = self.incl * lead
        self.excl = self.excl * lead
        self.tail = self.tail * jnp.where(second, 1.0, sibling)
        self.total = self.total * sibling
        self.half = 2 * h


def fold_map(both):
    return jnp.concatenate([fold2(both[:LANES]), fold2(both[LANES:])], axis=0)


def unfold_map(both):
    return jnp.concatenate([stack2(both[:HC]), stack2(both[HC:])], axis=0)


def unfold_wide(both):
    return jnp.concatenate([stack2(both[:, :LANES]), stack2(both[:, LANES:])], axis=1)


def lin_parts(key_b, value_b, decay_b, removal_b, small_ref, extra_ref):
    key = key_b.astype(F32)
    value = value_b.astype(F32)
    decay = jnp.exp(-jnp.exp(small_ref[0:1] + decay_b.astype(F32)) + extra_ref[...])
    removal = jax.nn.sigmoid(small_ref[1:2] + removal_b.astype(F32))
    unit = key * lax.rsqrt(head_sum(key * key) + key_eps)
    return key, value, decay, unit, unit * removal


def lin_map_kernel(*refs):
    pieces = refs[:8]
    gain_ref, w_ref, small_ref, extra_ref = refs[8:12]
    normed_ref, pack, sol_ref, pre_ref, map_ref = refs[12:17]
    extra_buf, sem = refs[17:]
    wide_w = extra_buf.shape[1]
    extra_move = pltpu.make_async_copy(extra_ref, extra_buf, sem)
    extra_move.start()
    rows = pieces[0].shape[0]
    at_y = lax.axis_index("y")
    core = lax.axis_index("c")
    gain = gain_ref[...]
    for j in range(len(pieces)):
        row = pieces[j][...].astype(F32)
        scale = lax.rsqrt(jnp.mean(row * row, axis=-1, keepdims=True) + rms_eps)
        source = lax.rem(at_y + (4 - j % 4), 4)
        which = core if j < 4 else 1 - core
        at = pl.multiple_of((2 * source + which) * rows, rows)
        normed_ref[pl.ds(at, rows), :] = (row * scale * gain).astype(BF16)

    def project(columns):
        out = jnp.dot(normed_ref[...], columns, preferred_element_type=F32).astype(BF16)
        return out[:, :LANES], out[:, LANES:]

    key_b, value_b = project(w_ref[:, : 2 * wide_w])
    decay_b, removal_b = project(w_ref[:, 2 * wide_w :])
    for j, part in enumerate((key_b, value_b, decay_b, removal_b)):
        pack[j] = part
    extra_move.wait()
    key, value, decay, unit, strike = lin_parts(
        key_b, value_b, decay_b, removal_b, small_ref, extra_buf
    )

    chunks = normed_ref.shape[0] // CH
    parts = [slice(b * CH, (b + 1) * CH) for b in range(chunks)]
    ident = eye(LANES)
    one = jnp.where(ident, 1.0, 0.0).astype(F32)
    dec = Decays(decay)
    inverse = [one] * chunks
    mix_key = [jnp.zeros((LANES, LANES), F32)] * chunks
    while dec.half < CH:
        left = -unit * dec.excl
        st = strike * dec.tail
        kt = key * dec.tail
        mask = level_mask(dec.half)
        lower = []
        for b, p in enumerate(parts):
            pairs = dot_pair(
                stack2(left[p]), jnp.concatenate([st[p], st[p], kt[p], kt[p]], axis=0), NT
            )
            lower.append(jnp.where(mask, pairs[:, :LANES], 0.0))
            mix_key[b] = jnp.where(mask, pairs[:, LANES:], mix_key[b])
        if dec.half == 1:
            inverse = [inverse[b] + lower[b] for b in range(chunks)]
        else:
            step = [dot_inv(lower[b], inverse[b]) for b in range(chunks)]
            inverse = [inverse[b] + dot_inv(inverse[b], step[b]) for b in range(chunks)]
        dec.widen()
    left = -unit * dec.excl
    st = strike * dec.tail
    kt = key * dec.tail
    v2 = [stack2(value[p]) for p in parts]
    pushed = [dot_map(mix_key[b], v2[b]) for b in range(chunks)]
    sol = [
        dot_map(inverse[b], jnp.concatenate([stack2(left[p]), pushed[b]], axis=1))
        for b, p in enumerate(parts)
    ]
    for b in range(chunks):
        sol_ref[b] = fold2(sol[b])
    trans, add = [], []
    for b, p in enumerate(parts):
        both = dot_map(sol[b], stack2(st[p]), TN)
        trans.append(both[:LANES] + jnp.where(ident, dec.total[p][0:1], 0.0))
        add.append(both[LANES:] + dot_map(v2[b], stack2(kt[p]), TN))
    prefix = jnp.concatenate([trans[0], add[0]], axis=0)
    for b in range(1, chunks):
        pre_ref[b - 1] = fold_map(prefix)
        prefix = dot_map(prefix, trans[b])
        prefix = prefix + jnp.concatenate([jnp.zeros_like(add[b]), add[b]], axis=0)
    map_ref[...] = fold_map(prefix).astype(map_ref.dtype)


def rope(values, cosine, sine):
    lane = lax.broadcasted_iota(jnp.int32, values.shape, 1)
    low = (lane % HC) < HC // 2
    ahead = pltpu.roll(values, LANES - HC // 2, 1)
    back = pltpu.roll(values, HC // 2, 1)
    return values * cosine + jnp.where(low, -ahead, back) * sine


def read_kernel(
    recept_ref, pack_ref, small_ref, extra_ref, sol_ref, pre_ref, base_ref, read_ref,
):
    recept = recept_ref[...].astype(F32)
    key, value, decay, _, strike = lin_parts(*(pack_ref[j] for j in range(4)), small_ref, extra_ref)
    ident = eye(LANES)
    chunks = recept.shape[0] // CH
    parts = [slice(b * CH, (b + 1) * CH) for b in range(chunks)]
    out_beta = [jnp.zeros((LANES, LANES), F32)] * chunks
    out_key = [jnp.zeros((LANES, LANES), F32)] * chunks

    def fill(r, s, k, mask):
        for b, p in enumerate(parts):
            pairs = dot_pair(stack2(r[p]), jnp.concatenate([s[p], s[p], k[p], k[p]], axis=0), NT)
            out_beta[b] = jnp.where(mask, pairs[:, :LANES], out_beta[b])
            out_key[b] = jnp.where(mask, pairs[:, LANES:], out_key[b])

    dec = Decays(decay)
    fill(recept, strike, key, ident)
    while dec.half < CH:
        fill(recept * dec.incl, strike * dec.tail, key * dec.tail, level_mask(dec.half))
        dec.widen()
    start = recept * dec.incl
    for b, p in enumerate(parts):
        both = dot_map(out_beta[b], unfold_wide(sol_ref[b]))
        read = stack2(start[p]) + both[:, :LANES]
        local = both[:, LANES:] + dot_map(out_key[b], stack2(value[p]))
        if b == 0:
            read_ref[p, :] = fold2(read)
            base_ref[p, :] = fold2(local)
        else:
            through = dot_map(read, unfold_map(pre_ref[b - 1]), NT)
            read_ref[p, :] = fold2(through[:, :LANES])
            base_ref[p, :] = fold2(through[:, LANES:] + local)


def late_kernel(*refs):
    normed_ref = refs[0]
    w_refs = refs[1:3]
    kvw_refs = refs[3:5]
    cos_ref, sin_ref = refs[5:7]
    recept_out, q_out, kv_out, rim_out, w_buf, kvw_buf, table, sems = refs[7:]
    width = w_refs[0].shape[1]
    narrow = kvw_refs[0].shape[0]
    moves = [(ref, kvw_buf.at[j * narrow : (j + 1) * narrow, :]) for j, ref in enumerate(kvw_refs)]
    moves += [(ref, table.at[j]) for j, ref in enumerate((cos_ref, sin_ref))]
    moves += [(ref, w_buf.at[:, j * width : (j + 1) * width]) for j, ref in enumerate(w_refs)]
    moves = [pltpu.make_async_copy(a, b, sems.at[j]) for j, (a, b) in enumerate(moves)]
    for move in moves:
        move.start()
    for move in moves[:2]:
        move.wait()
    raw = lax.dot_general(normed_ref[...], kvw_buf[...], NT, preferred_element_type=F32)
    raw = raw.astype(BF16).astype(F32)
    for move in moves[2:]:
        move.wait()
    cosine = table[0]
    sine = table[1]
    kv = jnp.where(head_masks(raw.shape[0]), rope(raw, cosine, sine), raw).astype(BF16)
    kv_out[...] = kv
    rim_out[...] = kv[kv.shape[0] - WINDOW :]
    out = jnp.dot(normed_ref[...], w_buf[...], preferred_element_type=F32).astype(BF16)
    recept_out[...] = out[:, :LANES]
    q = out[:, LANES:].astype(F32)
    q_out[...] = (rope(q, cosine, sine) * HC ** (-0.5)).astype(BF16)


def window_kernel(q_ref, kv_ref, rim_ref, small_ref, out_ref):
    q_all = q_ref[...].astype(F32)
    kv_all = jnp.concatenate([rim_ref[...], kv_ref[...]], axis=0)
    first = head_masks(WINDOW)
    seen = jnp.where(lax.axis_index(SP) == 0, WINDOW, 0)
    row = lax.broadcasted_iota(jnp.int32, (2 * WINDOW, 2 * WINDOW), 0) % WINDOW
    col = lax.broadcasted_iota(jnp.int32, (2 * WINDOW, 2 * WINDOW), 1)
    relative = WINDOW + row - col
    near = (relative >= 0) & (relative < WINDOW)
    head = lax.broadcasted_iota(jnp.int32, (2 * WINDOW, 1), 0) < WINDOW
    sinks = jnp.where(head, small_ref[3:4, 0:1], small_ref[3:4, HC : HC + 1])
    for b in range(q_all.shape[0] // WINDOW):
        q = q_all[b * WINDOW : (b + 1) * WINDOW]
        shifted = pltpu.roll(q, HC, 1)
        left = jnp.concatenate(
            [jnp.where(first, q, 0.0), jnp.where(first, shifted, 0.0)], axis=0
        ).astype(BF16)
        keys = kv_all[b * WINDOW : (b + 2) * WINDOW]
        valid = near & (col >= seen) if b == 0 else near
        scores = lax.dot_general(left, keys, NT, preferred_element_type=F32)
        scores = jnp.where(valid, scores, -jnp.inf)
        top = jnp.maximum(jnp.max(scores, axis=-1, keepdims=True), sinks)
        raised = jnp.exp(scores - top)
        total = jnp.sum(raised, axis=-1, keepdims=True) + jnp.exp(sinks - top)
        prob = (raised / total).astype(BF16)
        weighted = jnp.dot(prob, keys, preferred_element_type=F32)
        low = pltpu.roll(weighted[:WINDOW], HC, 1)
        out_ref[b * WINDOW : (b + 1) * WINDOW, :] = jnp.where(
            first, low, weighted[WINDOW:]
        ).astype(BF16)


def join_kernel(two_ref, one_ref, three_ref, own_ref, total_ref, before_ref, maps_ref):
    at = lax.axis_index("x")
    count = maps_ref.shape[0]
    for d, ref in enumerate((own_ref, one_ref, two_ref, three_ref)):
        maps_ref[lax.rem(at + (4 - d), 4)] = ref[...]
    total = unfold_map(maps_ref[0].astype(F32))
    ident = jnp.where(eye(LANES), 1.0, 0.0).astype(F32)
    before = jnp.concatenate([ident, jnp.zeros_like(ident)], axis=0)
    for k in range(1, count):
        before = jnp.where(at >= k, total, before)
        later = unfold_map(maps_ref[k])
        high, low = split(total)
        trans = later[:LANES].astype(BF16)
        total = jnp.dot(high, trans, preferred_element_type=F32)
        total = total + jnp.dot(low, trans, preferred_element_type=F32)
        total = total + jnp.concatenate(
            [jnp.zeros_like(ident), later[LANES:].astype(F32)], axis=0
        )
    before_ref[...] = before
    folded = fold_map(total).astype(BF16)
    for j in range(total_ref.shape[0]):
        total_ref[j] = folded


def final_kernel(
    maps_ref, before_ref, state_ref, base_ref, read_ref, small_ref, win_ref,
    mine_ref, other_ref,
):
    at = lax.axis_index("z")
    core = lax.axis_index("c")
    state = state_ref[...]
    for k in range(maps_ref.shape[0] - 1):
        both = maps_ref[k]
        high, low = split(state)
        moved = lax.dot_general(
            jnp.concatenate([high, low], axis=0), stack2(both[:HC]), NN,
            preferred_element_type=F32,
        )
        moved = moved[:LANES] + moved[LANES:] + stack2(both[HC:].astype(F32))
        state = jnp.where(at > k, moved, state)
    state = dot_map(state, before_ref[:LANES, :]) + before_ref[LANES:, :]
    reading = base_ref[...] + dot_map(read_ref[...], state, NT)
    centered = reading - head_sum(reading) * (1.0 / HC)
    spread = head_sum(centered * centered) * (1.0 / HC)
    lin = (centered * lax.rsqrt(spread + group_eps) * small_ref[2:3]).astype(BF16)
    left = jnp.concatenate([lin, win_ref[...]], axis=1)
    blocks = 4
    height = left.shape[0] // (2 * blocks)
    for j in range(blocks):
        even = left[2 * j * height : (2 * j + 1) * height]
        odd = left[(2 * j + 1) * height : (2 * j + 2) * height]
        mine_ref[j * height : (j + 1) * height, :] = jnp.where(core == 0, even, odd)
        other_ref[j * height : (j + 1) * height, :] = jnp.where(core == 0, odd, even)


def out_kernel(mine_ref, got_ref, w_ref, *outs):
    at_y = lax.axis_index("y")
    height = outs[0].shape[0]
    blocks = len(outs)

    def turned(ref):
        picked = [
            ref[pl.ds(pl.multiple_of(lax.rem(at_y + d, blocks) * height, height), height), :]
            for d in range(blocks)
        ]
        return jnp.concatenate(picked, axis=0)

    left = jnp.concatenate([turned(mine_ref), turned(got_ref)], axis=1)
    term = jnp.dot(left, w_ref[...], preferred_element_type=F32).astype(BF16)
    for d in range(blocks):
        outs[d][...] = term[d * height : (d + 1) * height]


def load_columns_kernel(*refs):
    count = len(refs) - 2
    out, sems = refs[count:]
    width = refs[0].shape[1]
    moves = [
        pltpu.make_async_copy(
            refs[j], out.at[:, j * width : (j + 1) * width], sems.at[j]
        )
        for j in range(count)
    ]
    for move in moves:
        move.start()
    for move in moves:
        move.wait()


def load_rows_kernel(*refs):
    count = len(refs) - 2
    out, sems = refs[count:]
    height = refs[0].shape[0]
    moves = [
        pltpu.make_async_copy(
            refs[j], out.at[j * height : (j + 1) * height, :], sems.at[j]
        )
        for j in range(count)
    ]
    for move in moves:
        move.start()
    for move in moves:
        move.wait()


VM = pl.BlockSpec(memory_space=pltpu.VMEM)
SM = pl.BlockSpec(memory_space=pltpu.SMEM)


AN = pl.BlockSpec(memory_space=pl.ANY)


def call(kernel, outs, args, smem=(), anys=(), slow=(), any_outs=(), scratch=(), limit=16, name=None, flops=1e9):
    specs = [SM if i in smem else AN if i in anys else VM for i in range(len(args))]
    args = [
        a if i in smem else pltpu.with_memory_space_constraint(
            a, pltpu.HBM if i in anys or i in slow else pltpu.VMEM
        )
        for i, a in enumerate(args)
    ]
    return pl.pallas_call(
        kernel,
        out_shape=outs,
        in_specs=specs,
        out_specs=(
            tuple(AN if i in any_outs else VM for i in range(len(outs)))
            if isinstance(outs, tuple)
            else VM
        ),
        scratch_shapes=list(scratch),
        name=name,
        compiler_params=pltpu.CompilerParams(vmem_limit_bytes=limit << 20),
        cost_estimate=pl.CostEstimate(flops=int(flops), transcendentals=0, bytes_accessed=1000000),
    )(*args)


def shape(dims, dtype):
    return pltpu.VMEM(dims, dtype)


def exchanged(array, axis):
    return lax.all_to_all(array, axis, split_axis=0, concat_axis=0, tiled=True)


def copies(array, axis):
    return jnp.broadcast_to(array, (lax.axis_size(axis), *array.shape))


def per_device(
    tokens_in, norm_gain, w_recept, w_key_lin, w_value_lin, w_decay, w_removal,
    decay_base, removal_base, decay_extra, initial_state, group_gain,
    w_query, w_key_win, w_value_win, sink_logit, w_out_linear, w_out_window,
):
    model = tokens_in.shape[1]
    count = decay_extra.shape[0]
    width = decay_extra.shape[1]
    chunks = count // CH
    sp_index = lax.axis_index(SP)
    swap = [(0, 1), (1, 0)]
    turn = lambda array, d: lax.ppermute(array, "y", [(i, (i + d) % 4) for i in range(4)])

    near = {0: tokens_in, **{d: turn(tokens_in, d) for d in (2, 1, 3)}}
    far = {d: lax.ppermute(near[d], "c", swap) for d in (0, 2, 1, 3)}

    inverse = theta_base ** (-jnp.arange(0, HC, 2, dtype=F32) / HC)
    positions = (sp_index * count + jnp.arange(count)).astype(F32)
    angle = positions[:, None] * jnp.tile(inverse, LANES // (HC // 2))[None, :]
    cosine = jnp.cos(angle)
    sine = jnp.sin(angle)
    small = jnp.stack([decay_base, removal_base, group_gain, jnp.repeat(sink_logit, HC)])
    zeros = jnp.zeros((HC, HC), F32)
    state0 = jnp.concatenate(
        [
            jnp.concatenate([initial_state[0], zeros], axis=1),
            jnp.concatenate([zeros, initial_state[1]], axis=1),
        ],
        axis=0,
    )

    row = lambda a: a.reshape(1, -1)
    w_out_other = [lax.ppermute(w, "c", swap) for w in (w_out_linear, w_out_window)]
    w_lin = call(
        load_columns_kernel,
        shape((model, 4 * width), BF16),
        (w_key_lin, w_value_lin, w_decay, w_removal),
        anys=range(4),
        scratch=(pltpu.SemaphoreType.DMA((4,)),),
        limit=4,
        flops=3e9,
        name="load_lin",
    )
    far[2], cosine, sine, state0, w_out_other, w_lin = lax.optimization_barrier(
        (far[2], cosine, sine, state0, w_out_other, w_lin)
    )
    pieces = tuple(near[d] for d in range(4)) + tuple(far[d] for d in range(4))
    rows = tokens_in.shape[0]
    normed, pack, sol, pre, own_map = call(
        lin_map_kernel,
        (
            shape((count, model), BF16),
            shape((4, count, width), BF16),
            shape((chunks, HC, 2 * LANES), F32),
            shape((chunks - 1, 2 * HC, LANES), F32),
            shape((2 * HC, LANES), BF16),
        ),
        (*pieces, row(norm_gain), w_lin, small, decay_extra),
        anys=(11,),
        scratch=(pltpu.VMEM((count, width), F32), pltpu.SemaphoreType.DMA),
        limit=12,
        name="lin_map",
    )
    maps_x = tuple(
        lax.ppermute(own_map, "x", [(i, (i + d) % 4) for i in range(4)]) if d else own_map
        for d in (2, 1, 3, 0)
    )

    recept, q, kv, rim_out = call(
        late_kernel,
        (*(shape((count, width), BF16) for _ in range(3)), shape((WINDOW, width), BF16)),
        (normed, w_recept, w_query, w_key_win.T, w_value_win.T, cosine, sine),
        anys=range(1, 7),
        scratch=(
            pltpu.VMEM((model, 2 * width), BF16),
            pltpu.VMEM((2 * w_key_win.shape[1], model), BF16),
            pltpu.VMEM((2, count, width), F32),
            pltpu.SemaphoreType.DMA((6,)),
        ),
        limit=8,
        name="late",
    )
    maps_x, rim_out = lax.optimization_barrier((maps_x, rim_out))
    steps = lax.axis_size("z") * lax.axis_size("x")
    rim = lax.ppermute(rim_out, SP, [(i, i + 1) for i in range(steps - 1)])

    total, before = call(
        join_kernel,
        (
            shape((lax.axis_size("z"), 2 * HC, LANES), BF16),
            shape((2 * LANES, LANES), F32),
        ),
        maps_x,
        scratch=(pltpu.VMEM((4, 2 * HC, LANES), BF16),),
        limit=4,
        name="join",
    )
    maps_z = exchanged(total, "z")

    base, read = call(
        read_kernel,
        (shape((count, LANES), F32), shape((count, LANES), F32)),
        (recept, pack, small, decay_extra, sol, pre),
        limit=8,
        name="read",
    )
    win = call(
        window_kernel,
        shape((count, LANES), BF16),
        (q, kv, rim, small),
        limit=4,
        name="window",
    )
    mine, theirs = call(
        final_kernel,
        (shape((count // 2, 2 * LANES), BF16), shape((count // 2, 2 * LANES), BF16)),
        (maps_z, before, state0, base, read, small, win),
        limit=8,
        name="final",
    )
    mine, theirs, w_out = lax.optimization_barrier(
        (mine, theirs, (w_out_linear, w_out_window, *w_out_other))
    )
    got = lax.ppermute(theirs, "c", swap)
    w_out = call(
        load_rows_kernel,
        shape((4 * width, model), BF16),
        w_out,
        anys=range(4),
        scratch=(pltpu.SemaphoreType.DMA((4,)),),
        limit=4,
        flops=3e9,
        name="load_out",
    )
    sums = call(
        out_kernel,
        tuple(shape((rows, model), BF16) for _ in range(4)),
        (mine, got, w_out),
        limit=8,
        name="out",
    )
    arrived = [turn(sums[d], d) for d in (2, 1, 3)]
    total_rows = sums[0].astype(F32)
    for part in arrived:
        total_rows = total_rows + part.astype(F32)
    return total_rows.astype(BF16)


def solution(mesh):
    grid = Mesh(mesh.devices.reshape(8, 4, 4, 2), ("z", "x", "y", "c"))
    return jax.shard_map(
        per_device,
        mesh=grid,
        in_specs=(
            P((*SP, *TP), None),
            P(),
            P(None, TP),
            P(None, TP),
            P(None, TP),
            P(None, TP),
            P(None, TP),
            P(TP),
            P(TP),
            P(SP, TP),
            P(TP, None, None),
            P(TP),
            P(None, TP),
            P(None, TP),
            P(None, TP),
            P(TP),
            P(TP, None),
            P(TP, None),
        ),
        out_specs=P((*SP, *TP), None),
        check_vma=False,
    )
```

```python
import jax
import jax.numpy as jnp
from jax import lax
from jax.experimental import pallas as pl
from jax.experimental.pallas import tpu as pltpu
from jax.sharding import Mesh
from jax.sharding import PartitionSpec as P

HC = 64
WINDOW = 128
CH = 64
LANES = 128
SP = ("z", "x")
TP = ("y", "c")

rms_eps = 1e-06
group_eps = 0.00064
key_eps = 1e-06
theta_base = 10000.0
F32 = jnp.float32
BF16 = jnp.bfloat16

NN = (((1,), (0,)), ((), ()))
NT = (((1,), (1,)), ((), ()))
TN = (((0,), (0,)), ((), ()))


def dot1(a, b, dims=NN):
    return lax.dot_general(a.astype(BF16), b.astype(BF16), dims, preferred_element_type=F32)


def split(a):
    high = a.astype(BF16)
    return high, (a - high.astype(F32)).astype(BF16)


def dot3(a, b, dims=NN):
    ah, al = split(a)
    bh, bl = split(b)
    d = lambda p, q: lax.dot_general(p, q, dims, preferred_element_type=F32)
    return d(ah, bh) + (d(ah, bl) + d(al, bh))


dot_pair = dot1
dot_inv = dot1
dot_map = dot3


def head_masks(rows):
    lane = lax.broadcasted_iota(jnp.int32, (rows, LANES), 1)
    first = lane < HC
    return first


def stack2(a):
    first = head_masks(a.shape[0])
    zero = jnp.zeros_like(a)
    return jnp.concatenate([jnp.where(first, a, zero), jnp.where(first, zero, a)], axis=0)


def fold2(a):
    half = a.shape[0] // 2
    return a[:half] + a[half:]


def head_sum(a):
    first = head_masks(a.shape[0])
    low = jnp.sum(jnp.where(first, a, 0.0), axis=-1, keepdims=True)
    high = jnp.sum(jnp.where(first, 0.0, a), axis=-1, keepdims=True)
    return jnp.where(first, low, high)


def eye(count):
    row = lax.broadcasted_iota(jnp.int32, (count, count), 0)
    col = lax.broadcasted_iota(jnp.int32, (count, count), 1)
    return row == col


def level_mask(half):
    row = lax.broadcasted_iota(jnp.int32, (LANES, LANES), 0)
    col = lax.broadcasted_iota(jnp.int32, (LANES, LANES), 1)
    step = 2 * half
    same = (row // step) == (col // step)
    return same & ((row % step) >= half) & ((col % step) < half)


class Decays:
    def __init__(self, decay):
        rows = decay.shape[0]
        self.row = lax.broadcasted_iota(jnp.int32, decay.shape, 0)
        self.rows = rows
        self.half = 1
        self.incl = decay
        self.excl = jnp.ones_like(decay)
        self.tail = jnp.ones_like(decay)
        self.total = decay

    def widen(self):
        h = self.half
        second = (self.row % (2 * h)) >= h
        back = pltpu.roll(self.total, h, 0)
        ahead = pltpu.roll(self.total, self.rows - h, 0)
        sibling = jnp.where(second, back, ahead)
        lead = jnp.where(second, sibling, 1.0)
        self.incl = self.incl * lead
        self.excl = self.excl * lead
        self.tail = self.tail * jnp.where(second, 1.0, sibling)
        self.total = self.total * sibling
        self.half = 2 * h


def fold_map(both):
    return jnp.concatenate([fold2(both[:LANES]), fold2(both[LANES:])], axis=0)


def unfold_map(both):
    return jnp.concatenate([stack2(both[:HC]), stack2(both[HC:])], axis=0)


def unfold_wide(both):
    return jnp.concatenate([stack2(both[:, :LANES]), stack2(both[:, LANES:])], axis=1)


def lin_parts(key_b, value_b, decay_b, removal_b, small_ref, extra_ref):
    key = key_b.astype(F32)
    value = value_b.astype(F32)
    decay = jnp.exp(-jnp.exp(small_ref[0:1] + decay_b.astype(F32)) + extra_ref[...])
    removal = jax.nn.sigmoid(small_ref[1:2] + removal_b.astype(F32))
    unit = key * lax.rsqrt(head_sum(key * key) + key_eps)
    return key, value, decay, unit, unit * removal


def norm_project(pieces, places, gain_ref, w_ref, normed_ref, proj_ref):
    rows = pieces[0].shape[0]
    gain = gain_ref[...]
    at_y = lax.axis_index("y")
    core = lax.axis_index("c")
    done = []
    starts = []
    for ref, (d, own) in zip(pieces, places):
        row = ref[...].astype(F32)
        scale = lax.rsqrt(jnp.mean(row * row, axis=-1, keepdims=True) + rms_eps)
        source = lax.rem(at_y + (4 - d), 4)
        which = core if own else 1 - core
        at = pl.multiple_of((2 * source + which) * rows, rows)
        normed = (row * scale * gain).astype(BF16)
        normed_ref[pl.ds(at, rows), :] = normed
        done.append(normed)
        starts.append(at)
    proj = jnp.dot(jnp.concatenate(done, axis=0), w_ref[...], preferred_element_type=F32)
    proj = proj.astype(BF16)
    for j, at in enumerate(starts):
        proj_ref[pl.ds(at, rows), :] = proj[j * rows : (j + 1) * rows]


def early_kernel(*refs):
    places = [(0, True), (0, False), (2, True), (2, False)]
    norm_project(refs[:4], places, *refs[4:])


def lin_map_kernel(*refs):
    places = [(1, True), (1, False), (3, True), (3, False)]
    pieces = refs[:4]
    gain_ref, w_ref, small_ref, extra_ref = refs[4:8]
    normed_ref, proj_ref, sol_ref, pre_ref, map_ref = refs[10:15]
    extra_buf, sem = refs[15:]
    wide_w = extra_buf.shape[1]
    extra_move = pltpu.make_async_copy(extra_ref, extra_buf, sem)
    extra_move.start()
    norm_project(pieces, places, gain_ref, w_ref, normed_ref, proj_ref)
    key_b, value_b, decay_b, removal_b = (
        proj_ref[:, j * wide_w : (j + 1) * wide_w] for j in range(4)
    )
    extra_move.wait()
    key, value, decay, unit, strike = lin_parts(
        key_b, value_b, decay_b, removal_b, small_ref, extra_buf
    )

    chunks = proj_ref.shape[0] // CH
    parts = [slice(b * CH, (b + 1) * CH) for b in range(chunks)]
    ident = eye(LANES)
    one = jnp.where(ident, 1.0, 0.0).astype(F32)
    dec = Decays(decay)
    inverse = [one] * chunks
    mix_key = [jnp.zeros((LANES, LANES), F32)] * chunks
    while dec.half < CH:
        left = -unit * dec.excl
        st = strike * dec.tail
        kt = key * dec.tail
        mask = level_mask(dec.half)
        lower = []
        for b, p in enumerate(parts):
            pairs = dot_pair(
                stack2(left[p]), jnp.concatenate([st[p], st[p], kt[p], kt[p]], axis=0), NT
            )
            lower.append(jnp.where(mask, pairs[:, :LANES], 0.0))
            mix_key[b] = jnp.where(mask, pairs[:, LANES:], mix_key[b])
        if dec.half == 1:
            inverse = [inverse[b] + lower[b] for b in range(chunks)]
        else:
            step = [dot_inv(lower[b], inverse[b]) for b in range(chunks)]
            inverse = [inverse[b] + dot_inv(inverse[b], step[b]) for b in range(chunks)]
        dec.widen()
    left = -unit * dec.excl
    st = strike * dec.tail
    kt = key * dec.tail
    v2 = [stack2(value[p]) for p in parts]
    pushed = [dot_map(mix_key[b], v2[b]) for b in range(chunks)]
    sol = [
        dot_map(inverse[b], jnp.concatenate([stack2(left[p]), pushed[b]], axis=1))
        for b, p in enumerate(parts)
    ]
    for b in range(chunks):
        sol_ref[b] = fold2(sol[b])
    trans, add = [], []
    for b, p in enumerate(parts):
        both = dot_map(sol[b], stack2(st[p]), TN)
        trans.append(both[:LANES] + jnp.where(ident, dec.total[p][0:1], 0.0))
        add.append(both[LANES:] + dot_map(v2[b], stack2(kt[p]), TN))
    prefix = jnp.concatenate([trans[0], add[0]], axis=0)
    for b in range(1, chunks):
        pre_ref[b - 1] = fold_map(prefix)
        prefix = dot_map(prefix, trans[b])
        prefix = prefix + jnp.concatenate([jnp.zeros_like(add[b]), add[b]], axis=0)
    map_ref[...] = fold_map(prefix).astype(map_ref.dtype)


def rope(values, cosine, sine):
    lane = lax.broadcasted_iota(jnp.int32, values.shape, 1)
    low = (lane % HC) < HC // 2
    ahead = pltpu.roll(values, LANES - HC // 2, 1)
    back = pltpu.roll(values, HC // 2, 1)
    return values * cosine + jnp.where(low, -ahead, back) * sine


def read_kernel(
    recept_ref, pack_ref, small_ref, extra_ref, sol_ref, pre_ref, wl_ref, ww_ref,
    base_ref, read_ref, w_ref, sems,
):
    height = wl_ref.shape[0]
    moves = [
        pltpu.make_async_copy(ref, w_ref.at[j * height : (j + 1) * height, :], sems.at[j])
        for j, ref in enumerate((wl_ref, ww_ref))
    ]
    for move in moves:
        move.start()
    recept = recept_ref[...].astype(F32)
    key, value, decay, _, strike = lin_parts(*(pack_ref[:, j * LANES : (j + 1) * LANES] for j in range(4)), small_ref, extra_ref)
    ident = eye(LANES)
    chunks = recept.shape[0] // CH
    parts = [slice(b * CH, (b + 1) * CH) for b in range(chunks)]
    out_beta = [jnp.zeros((LANES, LANES), F32)] * chunks
    out_key = [jnp.zeros((LANES, LANES), F32)] * chunks

    def fill(r, s, k, mask):
        for b, p in enumerate(parts):
            pairs = dot_pair(stack2(r[p]), jnp.concatenate([s[p], s[p], k[p], k[p]], axis=0), NT)
            out_beta[b] = jnp.where(mask, pairs[:, :LANES], out_beta[b])
            out_key[b] = jnp.where(mask, pairs[:, LANES:], out_key[b])

    dec = Decays(decay)
    fill(recept, strike, key, ident)
    while dec.half < CH:
        fill(recept * dec.incl, strike * dec.tail, key * dec.tail, level_mask(dec.half))
        dec.widen()
    start = recept * dec.incl
    for b, p in enumerate(parts):
        both = dot_map(out_beta[b], unfold_wide(sol_ref[b]))
        read = stack2(start[p]) + both[:, :LANES]
        local = both[:, LANES:] + dot_map(out_key[b], stack2(value[p]))
        if b == 0:
            read_ref[p, :] = fold2(read)
            base_ref[p, :] = fold2(local)
        else:
            through = dot_map(read, unfold_map(pre_ref[b - 1]), NT)
            read_ref[p, :] = fold2(through[:, :LANES])
            base_ref[p, :] = fold2(through[:, LANES:] + local)
    for move in moves:
        move.wait()


def late_kernel(*refs):
    normed_ref = refs[0]
    w_refs = refs[1:3]
    kvw_refs = refs[3:5]
    cos_ref, sin_ref = refs[5:7]
    recept_out, q_out, kv_out, rim_out, w_buf, kvw_buf, table, sems = refs[7:]
    width = w_refs[0].shape[1]
    narrow = kvw_refs[0].shape[0]
    moves = [(ref, kvw_buf.at[j * narrow : (j + 1) * narrow, :]) for j, ref in enumerate(kvw_refs)]
    moves += [(ref, table.at[j]) for j, ref in enumerate((cos_ref, sin_ref))]
    moves += [(ref, w_buf.at[:, j * width : (j + 1) * width]) for j, ref in enumerate(w_refs)]
    moves = [pltpu.make_async_copy(a, b, sems.at[j]) for j, (a, b) in enumerate(moves)]
    for move in moves:
        move.start()
    for move in moves[:2]:
        move.wait()
    raw = lax.dot_general(normed_ref[...], kvw_buf[...], NT, preferred_element_type=F32)
    raw = raw.astype(BF16).astype(F32)
    for move in moves[2:]:
        move.wait()
    cosine = table[0]
    sine = table[1]
    kv = jnp.where(head_masks(raw.shape[0]), rope(raw, cosine, sine), raw).astype(BF16)
    kv_out[...] = kv
    rim_out[...] = kv[kv.shape[0] - WINDOW :]
    out = jnp.dot(normed_ref[...], w_buf[...], preferred_element_type=F32).astype(BF16)
    recept_out[...] = out[:, :LANES]
    q = out[:, LANES:].astype(F32)
    q_out[...] = (rope(q, cosine, sine) * HC ** (-0.5)).astype(BF16)


def window_kernel(q_ref, kv_ref, rim_ref, small_ref, out_ref):
    q_all = q_ref[...].astype(F32)
    kv_all = jnp.concatenate([rim_ref[...], kv_ref[...]], axis=0)
    first = head_masks(WINDOW)
    seen = jnp.where(lax.axis_index(SP) == 0, WINDOW, 0)
    row = lax.broadcasted_iota(jnp.int32, (2 * WINDOW, 2 * WINDOW), 0) % WINDOW
    col = lax.broadcasted_iota(jnp.int32, (2 * WINDOW, 2 * WINDOW), 1)
    relative = WINDOW + row - col
    near = (relative >= 0) & (relative < WINDOW)
    head = lax.broadcasted_iota(jnp.int32, (2 * WINDOW, 1), 0) < WINDOW
    sinks = jnp.where(head, small_ref[3:4, 0:1], small_ref[3:4, HC : HC + 1])
    for b in range(q_all.shape[0] // WINDOW):
        q = q_all[b * WINDOW : (b + 1) * WINDOW]
        shifted = pltpu.roll(q, HC, 1)
        left = jnp.concatenate(
            [jnp.where(first, q, 0.0), jnp.where(first, shifted, 0.0)], axis=0
        ).astype(BF16)
        keys = kv_all[b * WINDOW : (b + 2) * WINDOW]
        valid = near & (col >= seen) if b == 0 else near
        scores = lax.dot_general(left, keys, NT, preferred_element_type=F32)
        scores = jnp.where(valid, scores, -jnp.inf)
        top = jnp.maximum(jnp.max(scores, axis=-1, keepdims=True), sinks)
        raised = jnp.exp(scores - top)
        total = jnp.sum(raised, axis=-1, keepdims=True) + jnp.exp(sinks - top)
        prob = (raised / total).astype(BF16)
        weighted = jnp.dot(prob, keys, preferred_element_type=F32)
        low = pltpu.roll(weighted[:WINDOW], HC, 1)
        out_ref[b * WINDOW : (b + 1) * WINDOW, :] = jnp.where(
            first, low, weighted[WINDOW:]
        ).astype(BF16)


def join_kernel(two_ref, one_ref, three_ref, own_ref, total_ref, before_ref, maps_ref):
    at = lax.axis_index("x")
    count = maps_ref.shape[0]
    for d, ref in enumerate((own_ref, one_ref, two_ref, three_ref)):
        maps_ref[lax.rem(at + (4 - d), 4)] = ref[...]
    total = unfold_map(maps_ref[0].astype(F32))
    ident = jnp.where(eye(LANES), 1.0, 0.0).astype(F32)
    before = jnp.concatenate([ident, jnp.zeros_like(ident)], axis=0)
    for k in range(1, count):
        before = jnp.where(at >= k, total, before)
        later = unfold_map(maps_ref[k])
        high, low = split(total)
        trans = later[:LANES].astype(BF16)
        total = jnp.dot(high, trans, preferred_element_type=F32)
        total = total + jnp.dot(low, trans, preferred_element_type=F32)
        total = total + jnp.concatenate(
            [jnp.zeros_like(ident), later[LANES:].astype(F32)], axis=0
        )
    before_ref[...] = before
    folded = fold_map(total).astype(BF16)
    for j in range(total_ref.shape[0]):
        total_ref[j] = folded


def final_kernel(
    maps_ref, before_ref, state_ref, base_ref, read_ref, small_ref, win_ref,
    mine_ref, other_ref,
):
    at = lax.axis_index("z")
    core = lax.axis_index("c")
    state = state_ref[...]
    for k in range(maps_ref.shape[0] - 1):
        both = maps_ref[k]
        high, low = split(state)
        moved = lax.dot_general(
            jnp.concatenate([high, low], axis=0), stack2(both[:HC]), NN,
            preferred_element_type=F32,
        )
        moved = moved[:LANES] + moved[LANES:] + stack2(both[HC:].astype(F32))
        state = jnp.where(at > k, moved, state)
    state = dot_map(state, before_ref[:LANES, :]) + before_ref[LANES:, :]
    reading = base_ref[...] + dot_map(read_ref[...], state, NT)
    centered = reading - head_sum(reading) * (1.0 / HC)
    spread = head_sum(centered * centered) * (1.0 / HC)
    lin = (centered * lax.rsqrt(spread + group_eps) * small_ref[2:3]).astype(BF16)
    left = jnp.concatenate([lin, win_ref[...]], axis=1)
    blocks = 4
    height = left.shape[0] // (2 * blocks)
    for j in range(blocks):
        even = left[2 * j * height : (2 * j + 1) * height]
        odd = left[(2 * j + 1) * height : (2 * j + 2) * height]
        mine_ref[j * height : (j + 1) * height, :] = jnp.where(core == 0, even, odd)
        other_ref[j * height : (j + 1) * height, :] = jnp.where(core == 0, odd, even)


def out_kernel(mine_ref, got_ref, own_ref, w_ref, *outs):
    at_y = lax.axis_index("y")
    height = outs[0].shape[0]
    blocks = len(outs)

    def turned(ref):
        picked = [
            ref[pl.ds(pl.multiple_of(lax.rem(at_y + d, blocks) * height, height), height), :]
            for d in range(blocks)
        ]
        return jnp.concatenate(picked, axis=0)

    term = jnp.dot(turned(mine_ref), own_ref[...], preferred_element_type=F32)
    term = term + jnp.dot(turned(got_ref), w_ref[...], preferred_element_type=F32)
    term = term.astype(BF16)
    for d in range(blocks):
        outs[d][...] = term[d * height : (d + 1) * height]


def load_columns_kernel(*refs):
    count = len(refs) - 2
    out, sems = refs[count:]
    width = refs[0].shape[1]
    moves = [
        pltpu.make_async_copy(
            refs[j], out.at[:, j * width : (j + 1) * width], sems.at[j]
        )
        for j in range(count)
    ]
    for move in moves:
        move.start()
    for move in moves:
        move.wait()


def load_rows_kernel(*refs):
    count = len(refs) - 2
    out, sems = refs[count:]
    height = refs[0].shape[0]
    moves = [
        pltpu.make_async_copy(
            refs[j], out.at[j * height : (j + 1) * height, :], sems.at[j]
        )
        for j in range(count)
    ]
    for move in moves:
        move.start()
    for move in moves:
        move.wait()


VM = pl.BlockSpec(memory_space=pltpu.VMEM)
SM = pl.BlockSpec(memory_space=pltpu.SMEM)


AN = pl.BlockSpec(memory_space=pl.ANY)


def call(kernel, outs, args, smem=(), anys=(), slow=(), any_outs=(), alias=None, scratch=(), limit=16, name=None, flops=1e9):
    specs = [SM if i in smem else AN if i in anys else VM for i in range(len(args))]
    args = [
        a if i in smem else pltpu.with_memory_space_constraint(
            a, pltpu.HBM if i in anys or i in slow else pltpu.VMEM
        )
        for i, a in enumerate(args)
    ]
    return pl.pallas_call(
        kernel,
        out_shape=outs,
        in_specs=specs,
        out_specs=(
            tuple(AN if i in any_outs else VM for i in range(len(outs)))
            if isinstance(outs, tuple)
            else VM
        ),
        scratch_shapes=list(scratch),
        input_output_aliases=alias or {},
        name=name,
        compiler_params=pltpu.CompilerParams(vmem_limit_bytes=limit << 20),
        cost_estimate=pl.CostEstimate(flops=int(flops), transcendentals=0, bytes_accessed=1000000),
    )(*args)


def shape(dims, dtype):
    return pltpu.VMEM(dims, dtype)


def exchanged(array, axis):
    return lax.all_to_all(array, axis, split_axis=0, concat_axis=0, tiled=True)


def copies(array, axis):
    return jnp.broadcast_to(array, (lax.axis_size(axis), *array.shape))


def per_device(
    tokens_in, norm_gain, w_recept, w_key_lin, w_value_lin, w_decay, w_removal,
    decay_base, removal_base, decay_extra, initial_state, group_gain,
    w_query, w_key_win, w_value_win, sink_logit, w_out_linear, w_out_window,
):
    model = tokens_in.shape[1]
    count = decay_extra.shape[0]
    width = decay_extra.shape[1]
    chunks = count // CH
    sp_index = lax.axis_index(SP)
    swap = [(0, 1), (1, 0)]
    turn = lambda array, d: lax.ppermute(array, "y", [(i, (i + d) % 4) for i in range(4)])

    near = {0: tokens_in, **{d: turn(tokens_in, d) for d in (2, 1, 3)}}
    far = {d: lax.ppermute(near[d], "c", swap) for d in (0, 2, 3)}

    inverse = theta_base ** (-jnp.arange(0, HC, 2, dtype=F32) / HC)
    positions = (sp_index * count + jnp.arange(count)).astype(F32)
    angle = positions[:, None] * jnp.tile(inverse, LANES // (HC // 2))[None, :]
    cosine = jnp.cos(angle)
    sine = jnp.sin(angle)
    small = jnp.stack([decay_base, removal_base, group_gain, jnp.repeat(sink_logit, HC)])
    zeros = jnp.zeros((HC, HC), F32)
    state0 = jnp.concatenate(
        [
            jnp.concatenate([initial_state[0], zeros], axis=1),
            jnp.concatenate([zeros, initial_state[1]], axis=1),
        ],
        axis=0,
    )

    row = lambda a: a.reshape(1, -1)
    w_out_other = [lax.ppermute(w, "c", swap) for w in (w_out_linear, w_out_window)]
    w_lin = call(
        load_columns_kernel,
        shape((model, 4 * width), BF16),
        (w_key_lin, w_value_lin, w_decay, w_removal),
        anys=range(4),
        scratch=(pltpu.SemaphoreType.DMA((4,)),),
        limit=4,
        flops=3e9,
        name="load_lin",
    )
    far[2], cosine, sine, state0, w_out_other, w_lin = lax.optimization_barrier(
        (far[2], cosine, sine, state0, w_out_other, w_lin)
    )
    rows = tokens_in.shape[0]
    far[1] = lax.ppermute(near[1], "c", swap)
    far_two, _, _ = lax.optimization_barrier((far[2], near[1], near[3]))
    normed, pack = call(
        early_kernel,
        (shape((count, model), BF16), shape((count, 4 * width), BF16)),
        (near[0], far[0], near[2], far_two, row(norm_gain), w_lin),
        limit=12,
        name="early",
    )
    normed, pack, sol, pre, own_map = call(
        lin_map_kernel,
        (
            shape((count, model), BF16),
            shape((count, 4 * width), BF16),
            shape((chunks, HC, 2 * LANES), F32),
            shape((chunks - 1, 2 * HC, LANES), F32),
            shape((2 * HC, LANES), BF16),
        ),
        (
            near[1], far[1], near[3], far[3], row(norm_gain), w_lin, small, decay_extra,
            normed, pack,
        ),
        anys=(7,),
        scratch=(pltpu.VMEM((count, width), F32), pltpu.SemaphoreType.DMA),
        alias={8: 0, 9: 1},
        limit=12,
        name="lin_map",
    )
    maps_x = tuple(
        lax.ppermute(own_map, "x", [(i, (i + d) % 4) for i in range(4)]) if d else own_map
        for d in (2, 1, 3, 0)
    )

    recept, q, kv, rim_out = call(
        late_kernel,
        (*(shape((count, width), BF16) for _ in range(3)), shape((WINDOW, width), BF16)),
        (normed, w_recept, w_query, w_key_win.T, w_value_win.T, cosine, sine),
        anys=range(1, 7),
        scratch=(
            pltpu.VMEM((model, 2 * width), BF16),
            pltpu.VMEM((2 * w_key_win.shape[1], model), BF16),
            pltpu.VMEM((2, count, width), F32),
            pltpu.SemaphoreType.DMA((6,)),
        ),
        limit=8,
        name="late",
    )
    maps_x, rim_out = lax.optimization_barrier((maps_x, rim_out))
    steps = lax.axis_size("z") * lax.axis_size("x")
    rim = lax.ppermute(rim_out, SP, [(i, i + 1) for i in range(steps - 1)])

    total, before = call(
        join_kernel,
        (
            shape((lax.axis_size("z"), 2 * HC, LANES), BF16),
            shape((2 * LANES, LANES), F32),
        ),
        maps_x,
        scratch=(pltpu.VMEM((4, 2 * HC, LANES), BF16),),
        limit=4,
        name="join",
    )
    maps_z = exchanged(total, "z")

    base, read, w_own = call(
        read_kernel,
        (
            shape((count, LANES), F32),
            shape((count, LANES), F32),
            shape((2 * width, model), BF16),
        ),
        (recept, pack, small, decay_extra, sol, pre, w_out_linear, w_out_window),
        anys=(6, 7),
        scratch=(pltpu.SemaphoreType.DMA((2,)),),
        limit=8,
        name="read",
    )
    win = call(
        window_kernel,
        shape((count, LANES), BF16),
        (q, kv, rim, small),
        limit=4,
        name="window",
    )
    mine, theirs = call(
        final_kernel,
        (shape((count // 2, 2 * LANES), BF16), shape((count // 2, 2 * LANES), BF16)),
        (maps_z, before, state0, base, read, small, win),
        limit=8,
        name="final",
    )
    mine, theirs, w_out = lax.optimization_barrier(
        (mine, theirs, tuple(w_out_other))
    )
    got = lax.ppermute(theirs, "c", swap)
    w_out = call(
        load_rows_kernel,
        shape((2 * width, model), BF16),
        w_out,
        anys=range(2),
        scratch=(pltpu.SemaphoreType.DMA((2,)),),
        limit=4,
        flops=3e9,
        name="load_out",
    )
    sums = call(
        out_kernel,
        tuple(shape((rows, model), BF16) for _ in range(4)),
        (mine, got, w_own, w_out),
        limit=8,
        name="out",
    )
    arrived = [turn(sums[d], d) for d in (2, 1, 3)]
    total_rows = sums[0].astype(F32)
    for part in arrived:
        total_rows = total_rows + part.astype(F32)
    return total_rows.astype(BF16)


def solution(mesh):
    grid = Mesh(mesh.devices.reshape(8, 4, 4, 2), ("z", "x", "y", "c"))
    return jax.shard_map(
        per_device,
        mesh=grid,
        in_specs=(
            P((*SP, *TP), None),
            P(),
            P(None, TP),
            P(None, TP),
            P(None, TP),
            P(None, TP),
            P(None, TP),
            P(TP),
            P(TP),
            P(SP, TP),
            P(TP, None, None),
            P(TP),
            P(None, TP),
            P(None, TP),
            P(None, TP),
            P(TP),
            P(TP, None),
            P(TP, None),
        ),
        out_specs=P((*SP, *TP), None),
        check_vma=False,
    )
```

```python
import jax
import jax.numpy as jnp
from jax import lax
from jax.experimental import pallas as pl
from jax.experimental.pallas import tpu as pltpu
from jax.sharding import Mesh
from jax.sharding import PartitionSpec as P

HC = 64
WINDOW = 128
CH = 64
LANES = 128
SP = ("z", "x")
TP = ("y", "c")

rms_eps = 1e-06
group_eps = 0.00064
key_eps = 1e-06
theta_base = 10000.0
F32 = jnp.float32
BF16 = jnp.bfloat16

NN = (((1,), (0,)), ((), ()))
NT = (((1,), (1,)), ((), ()))
TN = (((0,), (0,)), ((), ()))


def dot1(a, b, dims=NN):
    return lax.dot_general(a.astype(BF16), b.astype(BF16), dims, preferred_element_type=F32)


def split(a):
    high = a.astype(BF16)
    return high, (a - high.astype(F32)).astype(BF16)


def dot3(a, b, dims=NN):
    ah, al = split(a)
    bh, bl = split(b)
    d = lambda p, q: lax.dot_general(p, q, dims, preferred_element_type=F32)
    return d(ah, bh) + (d(ah, bl) + d(al, bh))


dot_pair = dot1
dot_inv = dot1
dot_map = dot3


def head_masks(rows):
    lane = lax.broadcasted_iota(jnp.int32, (rows, LANES), 1)
    first = lane < HC
    return first


def stack2(a):
    first = head_masks(a.shape[0])
    zero = jnp.zeros_like(a)
    return jnp.concatenate([jnp.where(first, a, zero), jnp.where(first, zero, a)], axis=0)


def fold2(a):
    half = a.shape[0] // 2
    return a[:half] + a[half:]


def head_sum(a):
    first = head_masks(a.shape[0])
    low = jnp.sum(jnp.where(first, a, 0.0), axis=-1, keepdims=True)
    high = jnp.sum(jnp.where(first, 0.0, a), axis=-1, keepdims=True)
    return jnp.where(first, low, high)


def eye(count):
    row = lax.broadcasted_iota(jnp.int32, (count, count), 0)
    col = lax.broadcasted_iota(jnp.int32, (count, count), 1)
    return row == col


def level_mask(half):
    row = lax.broadcasted_iota(jnp.int32, (LANES, LANES), 0)
    col = lax.broadcasted_iota(jnp.int32, (LANES, LANES), 1)
    step = 2 * half
    same = (row // step) == (col // step)
    return same & ((row % step) >= half) & ((col % step) < half)


class Decays:
    def __init__(self, decay):
        rows = decay.shape[0]
        self.row = lax.broadcasted_iota(jnp.int32, decay.shape, 0)
        self.rows = rows
        self.half = 1
        self.incl = decay
        self.excl = jnp.ones_like(decay)
        self.tail = jnp.ones_like(decay)
        self.total = decay

    def widen(self):
        h = self.half
        second = (self.row % (2 * h)) >= h
        back = pltpu.roll(self.total, h, 0)
        ahead = pltpu.roll(self.total, self.rows - h, 0)
        sibling = jnp.where(second, back, ahead)
        lead = jnp.where(second, sibling, 1.0)
        self.incl = self.incl * lead
        self.excl = self.excl * lead
        self.tail = self.tail * jnp.where(second, 1.0, sibling)
        self.total = self.total * sibling
        self.half = 2 * h


def fold_map(both):
    return jnp.concatenate([fold2(both[:LANES]), fold2(both[LANES:])], axis=0)


def unfold_map(both):
    return jnp.concatenate([stack2(both[:HC]), stack2(both[HC:])], axis=0)


def unfold_wide(both):
    return jnp.concatenate([stack2(both[:, :LANES]), stack2(both[:, LANES:])], axis=1)


def lin_parts(key_b, value_b, decay_b, removal_b, small_ref, extra_ref):
    key = key_b.astype(F32)
    value = value_b.astype(F32)
    decay = jnp.exp(-jnp.exp(small_ref[0:1] + decay_b.astype(F32)) + extra_ref[...])
    removal = jax.nn.sigmoid(small_ref[1:2] + removal_b.astype(F32))
    unit = key * lax.rsqrt(head_sum(key * key) + key_eps)
    return key, value, decay, unit, unit * removal


def norm_project(pieces, places, gain_ref, w_ref, normed_ref, proj_ref):
    rows = pieces[0].shape[0]
    gain = gain_ref[...]
    at_y = lax.axis_index("y")
    core = lax.axis_index("c")
    done = []
    starts = []
    for ref, (d, own) in zip(pieces, places):
        row = ref[...].astype(F32)
        scale = lax.rsqrt(jnp.mean(row * row, axis=-1, keepdims=True) + rms_eps)
        source = lax.rem(at_y + (4 - d), 4)
        which = core if own else 1 - core
        at = pl.multiple_of((2 * source + which) * rows, rows)
        normed = (row * scale * gain).astype(BF16)
        normed_ref[pl.ds(at, rows), :] = normed
        done.append(normed)
        starts.append(at)
    proj = jnp.dot(jnp.concatenate(done, axis=0), w_ref[...], preferred_element_type=F32)
    proj = proj.astype(BF16)
    for j, at in enumerate(starts):
        proj_ref[pl.ds(at, rows), :] = proj[j * rows : (j + 1) * rows]


def early_kernel(*refs):
    places = [(0, True), (0, False), (2, True), (2, False)]
    norm_project(refs[:4], places, *refs[4:])


def lin_map_kernel(*refs):
    places = [(1, True), (1, False), (3, True), (3, False)]
    pieces = refs[:4]
    gain_ref, w_ref, small_ref, extra_ref = refs[4:8]
    normed_ref, proj_ref, sol_ref, pre_ref, map_ref = refs[10:15]
    extra_buf, sem = refs[15:]
    wide_w = extra_buf.shape[1]
    extra_move = pltpu.make_async_copy(extra_ref, extra_buf, sem)
    extra_move.start()
    norm_project(pieces, places, gain_ref, w_ref, normed_ref, proj_ref)
    key_b, value_b, decay_b, removal_b = (
        proj_ref[:, j * wide_w : (j + 1) * wide_w] for j in range(4)
    )
    extra_move.wait()
    key, value, decay, unit, strike = lin_parts(
        key_b, value_b, decay_b, removal_b, small_ref, extra_buf
    )

    chunks = proj_ref.shape[0] // CH
    parts = [slice(b * CH, (b + 1) * CH) for b in range(chunks)]
    ident = eye(LANES)
    one = jnp.where(ident, 1.0, 0.0).astype(F32)
    dec = Decays(decay)
    inverse = [one] * chunks
    mix_key = [jnp.zeros((LANES, LANES), F32)] * chunks
    while dec.half < CH:
        left = -unit * dec.excl
        st = strike * dec.tail
        kt = key * dec.tail
        mask = level_mask(dec.half)
        lower = []
        for b, p in enumerate(parts):
            pairs = dot_pair(
                stack2(left[p]), jnp.concatenate([st[p], st[p], kt[p], kt[p]], axis=0), NT
            )
            lower.append(jnp.where(mask, pairs[:, :LANES], 0.0))
            mix_key[b] = jnp.where(mask, pairs[:, LANES:], mix_key[b])
        if dec.half == 1:
            inverse = [inverse[b] + lower[b] for b in range(chunks)]
        else:
            step = [dot_inv(lower[b], inverse[b]) for b in range(chunks)]
            inverse = [inverse[b] + dot_inv(inverse[b], step[b]) for b in range(chunks)]
        dec.widen()
    left = -unit * dec.excl
    st = strike * dec.tail
    kt = key * dec.tail
    v2 = [stack2(value[p]) for p in parts]
    pushed = [dot_map(mix_key[b], v2[b]) for b in range(chunks)]
    sol = [
        dot_map(inverse[b], jnp.concatenate([stack2(left[p]), pushed[b]], axis=1))
        for b, p in enumerate(parts)
    ]
    for b in range(chunks):
        sol_ref[b] = fold2(sol[b])
    trans, add = [], []
    for b, p in enumerate(parts):
        both = dot_map(sol[b], stack2(st[p]), TN)
        trans.append(both[:LANES] + jnp.where(ident, dec.total[p][0:1], 0.0))
        add.append(both[LANES:] + dot_map(v2[b], stack2(kt[p]), TN))
    prefix = jnp.concatenate([trans[0], add[0]], axis=0)
    for b in range(1, chunks):
        pre_ref[b - 1] = fold_map(prefix)
        prefix = dot_map(prefix, trans[b])
        prefix = prefix + jnp.concatenate([jnp.zeros_like(add[b]), add[b]], axis=0)
    map_ref[...] = fold_map(prefix).astype(map_ref.dtype)


def rope(values, cosine, sine):
    lane = lax.broadcasted_iota(jnp.int32, values.shape, 1)
    low = (lane % HC) < HC // 2
    ahead = pltpu.roll(values, LANES - HC // 2, 1)
    back = pltpu.roll(values, HC // 2, 1)
    return values * cosine + jnp.where(low, -ahead, back) * sine


def read_kernel(
    recept_ref, pack_ref, small_ref, extra_ref, sol_ref, pre_ref, wl_ref, ww_ref,
    base_ref, read_ref, w_ref, sems,
):
    height = wl_ref.shape[0]
    moves = [
        pltpu.make_async_copy(ref, w_ref.at[j * height : (j + 1) * height, :], sems.at[j])
        for j, ref in enumerate((wl_ref, ww_ref))
    ]
    for move in moves:
        move.start()
    recept = recept_ref[...].astype(F32)
    key, value, decay, _, strike = lin_parts(*(pack_ref[:, j * LANES : (j + 1) * LANES] for j in range(4)), small_ref, extra_ref)
    ident = eye(LANES)
    chunks = recept.shape[0] // CH
    parts = [slice(b * CH, (b + 1) * CH) for b in range(chunks)]
    out_beta = [jnp.zeros((LANES, LANES), F32)] * chunks
    out_key = [jnp.zeros((LANES, LANES), F32)] * chunks

    def fill(r, s, k, mask):
        for b, p in enumerate(parts):
            pairs = dot_pair(stack2(r[p]), jnp.concatenate([s[p], s[p], k[p], k[p]], axis=0), NT)
            out_beta[b] = jnp.where(mask, pairs[:, :LANES], out_beta[b])
            out_key[b] = jnp.where(mask, pairs[:, LANES:], out_key[b])

    dec = Decays(decay)
    fill(recept, strike, key, ident)
    while dec.half < CH:
        fill(recept * dec.incl, strike * dec.tail, key * dec.tail, level_mask(dec.half))
        dec.widen()
    start = recept * dec.incl
    for b, p in enumerate(parts):
        both = dot_map(out_beta[b], unfold_wide(sol_ref[b]))
        read = stack2(start[p]) + both[:, :LANES]
        local = both[:, LANES:] + dot_map(out_key[b], stack2(value[p]))
        if b == 0:
            read_ref[p, :] = fold2(read)
            base_ref[p, :] = fold2(local)
        else:
            through = dot_map(read, unfold_map(pre_ref[b - 1]), NT)
            read_ref[p, :] = fold2(through[:, :LANES])
            base_ref[p, :] = fold2(through[:, LANES:] + local)
    for move in moves:
        move.wait()


def late_kernel(*refs):
    normed_ref = refs[0]
    w_refs = refs[1:3]
    kvw_refs = refs[3:5]
    cos_ref, sin_ref = refs[5:7]
    recept_out, q_out, kv_out, rim_out, w_buf, kvw_buf, table, sems = refs[7:]
    width = w_refs[0].shape[1]
    narrow = kvw_refs[0].shape[0]
    moves = [(ref, kvw_buf.at[j * narrow : (j + 1) * narrow, :]) for j, ref in enumerate(kvw_refs)]
    moves += [(ref, table.at[j]) for j, ref in enumerate((cos_ref, sin_ref))]
    moves += [(ref, w_buf.at[:, j * width : (j + 1) * width]) for j, ref in enumerate(w_refs)]
    moves = [pltpu.make_async_copy(a, b, sems.at[j]) for j, (a, b) in enumerate(moves)]
    for move in moves:
        move.start()
    for move in moves[:2]:
        move.wait()
    raw = lax.dot_general(normed_ref[...], kvw_buf[...], NT, preferred_element_type=F32)
    raw = raw.astype(BF16).astype(F32)
    for move in moves[2:]:
        move.wait()
    cosine = table[0]
    sine = table[1]
    kv = jnp.where(head_masks(raw.shape[0]), rope(raw, cosine, sine), raw).astype(BF16)
    kv_out[...] = kv
    rim_out[...] = kv[kv.shape[0] - WINDOW :]
    out = jnp.dot(normed_ref[...], w_buf[...], preferred_element_type=F32).astype(BF16)
    recept_out[...] = out[:, :LANES]
    q = out[:, LANES:].astype(F32)
    q_out[...] = (rope(q, cosine, sine) * HC ** (-0.5)).astype(BF16)


def window_kernel(q_ref, kv_ref, rim_ref, small_ref, wl_ref, ww_ref, out_ref, w_ref, sems):
    height = wl_ref.shape[0]
    moves = [
        pltpu.make_async_copy(ref, w_ref.at[j * height : (j + 1) * height, :], sems.at[j])
        for j, ref in enumerate((wl_ref, ww_ref))
    ]
    for move in moves:
        move.start()
    q_all = q_ref[...].astype(F32)
    kv_all = jnp.concatenate([rim_ref[...], kv_ref[...]], axis=0)
    first = head_masks(WINDOW)
    seen = jnp.where(lax.axis_index(SP) == 0, WINDOW, 0)
    row = lax.broadcasted_iota(jnp.int32, (2 * WINDOW, 2 * WINDOW), 0) % WINDOW
    col = lax.broadcasted_iota(jnp.int32, (2 * WINDOW, 2 * WINDOW), 1)
    relative = WINDOW + row - col
    near = (relative >= 0) & (relative < WINDOW)
    head = lax.broadcasted_iota(jnp.int32, (2 * WINDOW, 1), 0) < WINDOW
    sinks = jnp.where(head, small_ref[3:4, 0:1], small_ref[3:4, HC : HC + 1])
    for b in range(q_all.shape[0] // WINDOW):
        q = q_all[b * WINDOW : (b + 1) * WINDOW]
        shifted = pltpu.roll(q, HC, 1)
        left = jnp.concatenate(
            [jnp.where(first, q, 0.0), jnp.where(first, shifted, 0.0)], axis=0
        ).astype(BF16)
        keys = kv_all[b * WINDOW : (b + 2) * WINDOW]
        valid = near & (col >= seen) if b == 0 else near
        scores = lax.dot_general(left, keys, NT, preferred_element_type=F32)
        scores = jnp.where(valid, scores, -jnp.inf)
        top = jnp.maximum(jnp.max(scores, axis=-1, keepdims=True), sinks)
        raised = jnp.exp(scores - top)
        total = jnp.sum(raised, axis=-1, keepdims=True) + jnp.exp(sinks - top)
        prob = (raised / total).astype(BF16)
        weighted = jnp.dot(prob, keys, preferred_element_type=F32)
        low = pltpu.roll(weighted[:WINDOW], HC, 1)
        out_ref[b * WINDOW : (b + 1) * WINDOW, :] = jnp.where(
            first, low, weighted[WINDOW:]
        ).astype(BF16)
    for move in moves:
        move.wait()


def join_kernel(two_ref, one_ref, three_ref, own_ref, total_ref, before_ref, maps_ref):
    at = lax.axis_index("x")
    count = maps_ref.shape[0]
    for d, ref in enumerate((own_ref, one_ref, two_ref, three_ref)):
        maps_ref[lax.rem(at + (4 - d), 4)] = ref[...]
    total = unfold_map(maps_ref[0].astype(F32))
    ident = jnp.where(eye(LANES), 1.0, 0.0).astype(F32)
    before = jnp.concatenate([ident, jnp.zeros_like(ident)], axis=0)
    for k in range(1, count):
        before = jnp.where(at >= k, total, before)
        later = unfold_map(maps_ref[k])
        high, low = split(total)
        trans = later[:LANES].astype(BF16)
        total = jnp.dot(high, trans, preferred_element_type=F32)
        total = total + jnp.dot(low, trans, preferred_element_type=F32)
        total = total + jnp.concatenate(
            [jnp.zeros_like(ident), later[LANES:].astype(F32)], axis=0
        )
    before_ref[...] = before
    folded = fold_map(total).astype(BF16)
    for j in range(total_ref.shape[0]):
        total_ref[j] = folded


def final_kernel(
    maps_ref, before_ref, state_ref, base_ref, read_ref, small_ref, win_ref,
    mine_ref, other_ref,
):
    at = lax.axis_index("z")
    core = lax.axis_index("c")
    state = state_ref[...]
    for k in range(maps_ref.shape[0] - 1):
        both = maps_ref[k]
        high, low = split(state)
        moved = lax.dot_general(
            jnp.concatenate([high, low], axis=0), stack2(both[:HC]), NN,
            preferred_element_type=F32,
        )
        moved = moved[:LANES] + moved[LANES:] + stack2(both[HC:].astype(F32))
        state = jnp.where(at > k, moved, state)
    state = dot_map(state, before_ref[:LANES, :]) + before_ref[LANES:, :]
    reading = base_ref[...] + dot_map(read_ref[...], state, NT)
    centered = reading - head_sum(reading) * (1.0 / HC)
    spread = head_sum(centered * centered) * (1.0 / HC)
    lin = (centered * lax.rsqrt(spread + group_eps) * small_ref[2:3]).astype(BF16)
    left = jnp.concatenate([lin, win_ref[...]], axis=1)
    blocks = 4
    height = left.shape[0] // (2 * blocks)
    for j in range(blocks):
        even = left[2 * j * height : (2 * j + 1) * height]
        odd = left[(2 * j + 1) * height : (2 * j + 2) * height]
        mine_ref[j * height : (j + 1) * height, :] = jnp.where(core == 0, even, odd)
        other_ref[j * height : (j + 1) * height, :] = jnp.where(core == 0, odd, even)


def out_kernel(mine_ref, got_ref, own_ref, w_ref, *outs):
    at_y = lax.axis_index("y")
    height = outs[0].shape[0]
    blocks = len(outs)

    def turned(ref):
        picked = [
            ref[pl.ds(pl.multiple_of(lax.rem(at_y + d, blocks) * height, height), height), :]
            for d in range(blocks)
        ]
        return jnp.concatenate(picked, axis=0)

    term = jnp.dot(turned(mine_ref), own_ref[...], preferred_element_type=F32)
    term = term + jnp.dot(turned(got_ref), w_ref[...], preferred_element_type=F32)
    term = term.astype(BF16)
    for d in range(blocks):
        outs[d][...] = term[d * height : (d + 1) * height]


def load_columns_kernel(*refs):
    count = len(refs) - 2
    out, sems = refs[count:]
    width = refs[0].shape[1]
    moves = [
        pltpu.make_async_copy(
            refs[j], out.at[:, j * width : (j + 1) * width], sems.at[j]
        )
        for j in range(count)
    ]
    for move in moves:
        move.start()
    for move in moves:
        move.wait()


VM = pl.BlockSpec(memory_space=pltpu.VMEM)
SM = pl.BlockSpec(memory_space=pltpu.SMEM)


AN = pl.BlockSpec(memory_space=pl.ANY)


def call(kernel, outs, args, smem=(), anys=(), slow=(), any_outs=(), alias=None, scratch=(), limit=16, name=None, flops=1e9):
    specs = [SM if i in smem else AN if i in anys else VM for i in range(len(args))]
    args = [
        a if i in smem else pltpu.with_memory_space_constraint(
            a, pltpu.HBM if i in anys or i in slow else pltpu.VMEM
        )
        for i, a in enumerate(args)
    ]
    return pl.pallas_call(
        kernel,
        out_shape=outs,
        in_specs=specs,
        out_specs=(
            tuple(AN if i in any_outs else VM for i in range(len(outs)))
            if isinstance(outs, tuple)
            else VM
        ),
        scratch_shapes=list(scratch),
        input_output_aliases=alias or {},
        name=name,
        compiler_params=pltpu.CompilerParams(vmem_limit_bytes=limit << 20),
        cost_estimate=pl.CostEstimate(flops=int(flops), transcendentals=0, bytes_accessed=1000000),
    )(*args)


def shape(dims, dtype):
    return pltpu.VMEM(dims, dtype)


def exchanged(array, axis):
    return lax.all_to_all(array, axis, split_axis=0, concat_axis=0, tiled=True)


def copies(array, axis):
    return jnp.broadcast_to(array, (lax.axis_size(axis), *array.shape))


def per_device(
    tokens_in, norm_gain, w_recept, w_key_lin, w_value_lin, w_decay, w_removal,
    decay_base, removal_base, decay_extra, initial_state, group_gain,
    w_query, w_key_win, w_value_win, sink_logit, w_out_linear, w_out_window,
):
    model = tokens_in.shape[1]
    count = decay_extra.shape[0]
    width = decay_extra.shape[1]
    chunks = count // CH
    sp_index = lax.axis_index(SP)
    swap = [(0, 1), (1, 0)]
    turn = lambda array, d: lax.ppermute(array, "y", [(i, (i + d) % 4) for i in range(4)])

    near = {0: tokens_in, **{d: turn(tokens_in, d) for d in (2, 1, 3)}}
    far = {d: lax.ppermute(near[d], "c", swap) for d in (0, 2, 3)}

    inverse = theta_base ** (-jnp.arange(0, HC, 2, dtype=F32) / HC)
    positions = (sp_index * count + jnp.arange(count)).astype(F32)
    angle = positions[:, None] * jnp.tile(inverse, LANES // (HC // 2))[None, :]
    cosine = jnp.cos(angle)
    sine = jnp.sin(angle)
    small = jnp.stack([decay_base, removal_base, group_gain, jnp.repeat(sink_logit, HC)])
    zeros = jnp.zeros((HC, HC), F32)
    state0 = jnp.concatenate(
        [
            jnp.concatenate([initial_state[0], zeros], axis=1),
            jnp.concatenate([zeros, initial_state[1]], axis=1),
        ],
        axis=0,
    )

    row = lambda a: a.reshape(1, -1)
    w_out_other = [lax.ppermute(w, "c", swap) for w in (w_out_linear, w_out_window)]
    w_lin = call(
        load_columns_kernel,
        shape((model, 4 * width), BF16),
        (w_key_lin, w_value_lin, w_decay, w_removal),
        anys=range(4),
        scratch=(pltpu.SemaphoreType.DMA((4,)),),
        limit=4,
        flops=3e9,
        name="load_lin",
    )
    far[2], cosine, sine, state0, w_out_other, w_lin = lax.optimization_barrier(
        (far[2], cosine, sine, state0, w_out_other, w_lin)
    )
    rows = tokens_in.shape[0]
    far[1] = lax.ppermute(near[1], "c", swap)
    far_two, _, _ = lax.optimization_barrier((far[2], near[1], near[3]))
    normed, pack = call(
        early_kernel,
        (shape((count, model), BF16), shape((count, 4 * width), BF16)),
        (near[0], far[0], near[2], far_two, row(norm_gain), w_lin),
        limit=12,
        name="early",
    )
    normed, pack, sol, pre, own_map = call(
        lin_map_kernel,
        (
            shape((count, model), BF16),
            shape((count, 4 * width), BF16),
            shape((chunks, HC, 2 * LANES), F32),
            shape((chunks - 1, 2 * HC, LANES), F32),
            shape((2 * HC, LANES), BF16),
        ),
        (
            near[1], far[1], near[3], far[3], row(norm_gain), w_lin, small, decay_extra,
            normed, pack,
        ),
        anys=(7,),
        scratch=(pltpu.VMEM((count, width), F32), pltpu.SemaphoreType.DMA),
        alias={8: 0, 9: 1},
        limit=12,
        name="lin_map",
    )
    maps_x = tuple(
        lax.ppermute(own_map, "x", [(i, (i + d) % 4) for i in range(4)]) if d else own_map
        for d in (2, 1, 3, 0)
    )

    recept, q, kv, rim_out = call(
        late_kernel,
        (*(shape((count, width), BF16) for _ in range(3)), shape((WINDOW, width), BF16)),
        (normed, w_recept, w_query, w_key_win.T, w_value_win.T, cosine, sine),
        anys=range(1, 7),
        scratch=(
            pltpu.VMEM((model, 2 * width), BF16),
            pltpu.VMEM((2 * w_key_win.shape[1], model), BF16),
            pltpu.VMEM((2, count, width), F32),
            pltpu.SemaphoreType.DMA((6,)),
        ),
        limit=8,
        name="late",
    )
    maps_x, rim_out = lax.optimization_barrier((maps_x, rim_out))
    steps = lax.axis_size("z") * lax.axis_size("x")
    rim = lax.ppermute(rim_out, SP, [(i, i + 1) for i in range(steps - 1)])

    total, before = call(
        join_kernel,
        (
            shape((lax.axis_size("z"), 2 * HC, LANES), BF16),
            shape((2 * LANES, LANES), F32),
        ),
        maps_x,
        scratch=(pltpu.VMEM((4, 2 * HC, LANES), BF16),),
        limit=4,
        name="join",
    )
    maps_z = exchanged(total, "z")

    base, read, w_own = call(
        read_kernel,
        (
            shape((count, LANES), F32),
            shape((count, LANES), F32),
            shape((2 * width, model), BF16),
        ),
        (recept, pack, small, decay_extra, sol, pre, w_out_linear, w_out_window),
        anys=(6, 7),
        scratch=(pltpu.SemaphoreType.DMA((2,)),),
        limit=8,
        name="read",
    )
    win, w_out = call(
        window_kernel,
        (shape((count, LANES), BF16), shape((2 * width, model), BF16)),
        (q, kv, rim, small, *w_out_other),
        anys=(4, 5),
        scratch=(pltpu.SemaphoreType.DMA((2,)),),
        limit=4,
        name="window",
    )
    mine, theirs = call(
        final_kernel,
        (shape((count // 2, 2 * LANES), BF16), shape((count // 2, 2 * LANES), BF16)),
        (maps_z, before, state0, base, read, small, win),
        limit=8,
        name="final",
    )
    got = lax.ppermute(theirs, "c", swap)
    sums = call(
        out_kernel,
        tuple(shape((rows, model), BF16) for _ in range(4)),
        (mine, got, w_own, w_out),
        limit=8,
        name="out",
    )
    arrived = [turn(sums[d], d) for d in (2, 1, 3)]
    total_rows = sums[0].astype(F32)
    for part in arrived:
        total_rows = total_rows + part.astype(F32)
    return total_rows.astype(BF16)


def solution(mesh):
    grid = Mesh(mesh.devices.reshape(8, 4, 4, 2), ("z", "x", "y", "c"))
    return jax.shard_map(
        per_device,
        mesh=grid,
        in_specs=(
            P((*SP, *TP), None),
            P(),
            P(None, TP),
            P(None, TP),
            P(None, TP),
            P(None, TP),
            P(None, TP),
            P(TP),
            P(TP),
            P(SP, TP),
            P(TP, None, None),
            P(TP),
            P(None, TP),
            P(None, TP),
            P(None, TP),
            P(TP),
            P(TP, None),
            P(TP, None),
        ),
        out_specs=P((*SP, *TP), None),
        check_vma=False,
    )
```
